32 devices in a mesh: grp: 2 (over y), fs: 4 (over z), tp: 4 (over x, core).
Axes of the slice: x: 2, y: 2, z: 4, core: 2. Of those that a mesh axis runs over, the one named last changes fastest.
Arguments:
- tokens: bfloat16 [1536, 2048], P(('grp', 'fs'), 'tp'), parts along dimension 0, may hold values from -40 to 40
- routes: int32 [1536, 2], P(('grp', 'fs')), parts along dimension 0, may hold values from 0 to 3, all different within a row; in each aligned block of 192 rows (0 to 191, 192 to 383, ...) at most 112 rows name the same one
- routing_weight: float32 [1536, 2], P(('grp', 'fs')), parts along dimension 0, may hold values from 0.1 to 0.6
- norm_gain_vector: float32 [2048], P('tp'), may hold values from 0.1 to 1.9
- expert_gate: float32 [4, 512, 2048], P(None, 'fs', 'tp'), may hold values from -0.125 to 0.125
- expert_up: float32 [4, 512, 2048], P(None, 'fs', 'tp'), may hold values from -0.125 to 0.125
- expert_down: float32 [4, 512, 2048], P(None, 'fs', 'tp'), may hold values from -0.25 to 0.25
- shared_gate: float32 [512, 2048], P('fs', 'tp'), may hold values from -0.125 to 0.125
- shared_up: float32 [512, 2048], P('fs', 'tp'), may hold values from -0.125 to 0.125
- shared_down: float32 [512, 2048], P('fs', 'tp'), may hold values from -0.25 to 0.25
Outputs:
- mixed: bfloat16 [1536, 2048], P(('grp', 'fs'), 'tp'), parts along dimension 0
- gate_served: bfloat16 [8, 512, 2048], P(('grp', 'fs'), None, 'tp'), parts along dimension 0
- up_served: bfloat16 [8, 512, 2048], P(('grp', 'fs'), None, 'tp'), parts along dimension 0
- down_served: bfloat16 [8, 512, 2048], P(('grp', 'fs'), None, 'tp'), parts along dimension 0
- shared_gate_served: bfloat16 [1024, 2048], P('grp', 'tp'), parts along dimension 0
- shared_up_served: bfloat16 [1024, 2048], P('grp', 'tp'), parts along dimension 0
- shared_down_served: bfloat16 [1024, 2048], P('grp', 'tp'), parts along dimension 0
The draws below stay inside these ranges and needn't reach their ends.
There are 2 independent parts, one for each index of `grp`. The reference program is written for one: setup_inputs(seed, part) draws one part's arguments, and reference() takes and returns one part's arrays. A program takes and returns all parts, laid end to end along the dimension named above; an argument that names none is the same for every part. Nothing has to cross between parts.
Inputs may be any that keep to these rules, and one draw needn't show every extreme that they name: `routes`: each row names 2 different experts. In each aligned block of 192 rows no expert is named by more than 112 rows, and in some block an expert is named by exactly 112 rows.
All inputs are finite; a program needn't handle non-finite values.
Results may differ from the reference program's by a relative error of at most 0.022.
Values may be sent and summed in bfloat16 or wider, within the bound.
A program may use at most 64 MiB of HBM per device.

```python
import math
import jax
import jax.numpy as jnp
import numpy as np
from jax import lax

D = 2048
FF = 512
SFF = 512
TOK_G = 192
EXPERTS = 4
TOPK = 2
CAP = 112
TOKENS = 768
N_FS = 4
N_TP = 4


def draw_tokens(key, part):
    base_key = jax.random.fold_in(key, 11)
    first, second = jax.random.split(base_key, 2)
    column = jnp.arange(D).astype(jnp.float32)
    trend = 1.0 + 2.0 * column / (D - 1)
    rough = jnp.exp(jax.random.uniform(second, (D,), jnp.float32) * jnp.log(10.0))
    scales = trend * rough
    scales = scales / jnp.sqrt(jnp.mean(scales * scales))
    values = jax.random.normal(first, (TOKENS, D), jnp.float32) * scales[None, :]
    return jnp.clip(values, -40.0, 40.0).astype(jnp.bfloat16)


def shard_levels(stream_key, extent, shards, smallest, top_value):
    def one(dim, parts):
        steps = jax.random.uniform(jax.random.fold_in(jax.random.fold_in(stream_key, 6), dim), (parts,), jnp.float32, smallest / len(shards), top_value / len(shards))
        return jnp.repeat(jnp.exp(steps), extent[dim] // parts).reshape((-1,) + (1,) * (len(extent) - dim - 1))

    factor_of = one(*shards[0])
    for cut in shards[1:]:
        factor_of = factor_of * one(*cut)
    return factor_of


def deal_out(key, own, number, rows, amount, top, most, slope):
    order = jax.random.permutation(key, amount)
    packed, usual = portions_of(amount, rows * top, most, slope, True), portions_of(amount, rows * top, most, slope, False)
    places = jnp.arange(amount)

    def named(sizes, rotation):
        used = int((sizes > 0).sum())
        fixed = max(1, used // 4)
        moved = fixed + (places - fixed + rotation * (used - fixed)) % max(1, amount - fixed)
        return jnp.zeros((amount,), jnp.int32).at[order[jnp.where(places < fixed, places, moved)]].set(jnp.asarray(sizes, jnp.int32))

    sizes = jnp.where(number % 4 == 0, named(packed, number // 4), named(usual, number - number // 4 - 1))
    mixed = jax.random.permutation(jax.random.fold_in(own, 3), amount)
    giver, taker = mixed[0:amount // 2 * 2:2], mixed[1:amount // 2 * 2:2]
    margin = jnp.minimum(sizes[giver] - 1, most - sizes[taker]) // 2
    margin = jnp.where((giver == order[0]) | (taker == order[0]) | (sizes[taker] == 0), 0, jnp.maximum(margin, 0))
    moved = jax.random.randint(jax.random.fold_in(own, 4), (amount // 2,), 0, 1 << 20) % (margin + 1)
    sizes = sizes.at[giver].add(-moved).at[taker].add(moved)
    labels = jnp.searchsorted(jnp.cumsum(sizes), jnp.arange(rows * top), side="right").astype(jnp.int32)
    grid = labels.reshape(top, rows).T
    grid = grid[jax.random.permutation(jax.random.fold_in(own, 1), rows)]
    rotation = jax.random.randint(jax.random.fold_in(own, 2), (rows, 1), 0, top)
    return jnp.take_along_axis(grid, (jnp.arange(top)[None, :] + rotation) % top, axis=1)


def portions_of(count, total, most, slope, full):
    weights = [(1 << 20) // math.isqrt(standing ** slope) + 1 for standing in range(1, count + 1)]
    largest = most if full else min(most, max(-(-total // count), total * weights[0] // sum(weights)))
    least = 1 if total - largest >= count - 1 else 0
    counts, spare = [largest] + [least] * (count - 1), total - largest - least * (count - 1)
    while spare > 0:
        candidates = [i for i in range(1, count) if counts[i] < largest] or [i for i in range(1, count) if counts[i] < most]
        mass, left = sum([weights[i] for i in candidates]), spare
        for i in candidates:
            extra = min(most - counts[i], max(1, left * weights[i] // mass), spare)
            counts[i] = counts[i] + extra
            spare = spare - extra
    return np.array(counts)


def noise(key, dims, spread, reach, cuts=(), held_as=jnp.bfloat16):
    drawn = jax.random.normal(key, dims, jnp.float32) * spread
    if len(cuts) > 0:
        drawn = shard_levels(key, dims, cuts, -0.22, 0.18) * drawn
    return jnp.clip(drawn, min=-reach, max=reach).astype(held_as)


def setup_inputs(seed: int = 0, part: int = 0) -> dict:
    splits = jax.random.split(jax.random.key(seed), 11)
    part_splits = jax.random.split(jax.random.fold_in(splits[10], part), 11)
    tokens = draw_tokens(jax.random.fold_in(jax.random.fold_in(splits[10], part), 71), part)
    routes_keys = jax.random.split(jax.random.fold_in(part_splits[1], 1), TOKENS // TOK_G)
    routes_turns = jax.random.permutation(jax.random.fold_in(part_splits[1], 3), TOKENS // TOK_G)
    routes = jax.vmap(lambda own, number: deal_out(jax.random.fold_in(part_splits[1], 2), own, number, TOK_G, EXPERTS, TOPK, CAP, 1))(routes_keys, routes_turns).reshape((TOKENS, TOPK))
    routing_weight = jnp.clip(0.1 + 0.5 * jax.random.uniform(part_splits[2], (TOKENS, TOPK), jnp.float32) ** shard_levels(part_splits[2], (TOKENS, TOPK), ((0, 4),), -0.2, 0.2), 0.1, 0.6)
    norm_gain_vector = jnp.clip(1.0 + 0.18 * jax.random.normal(splits[3], (D,), jnp.float32), 0.1, 1.9)
    expert_gate = noise(splits[4], (EXPERTS, FF, D), D ** -0.5, 0.125, ((1, 4), (2, 4)), jnp.float32)
    expert_up = noise(splits[5], (EXPERTS, FF, D), D ** -0.5, 0.125, ((1, 4), (2, 4)), jnp.float32)
    expert_down = noise(splits[6], (EXPERTS, FF, D), FF ** -0.5, 0.25, ((1, 4), (2, 4)), jnp.float32)
    shared_gate = noise(splits[7], (SFF, D), D ** -0.5, 0.125, ((0, 4), (1, 4)), jnp.float32)
    shared_up = noise(splits[8], (SFF, D), D ** -0.5, 0.125, ((0, 4), (1, 4)), jnp.float32)
    shared_down = noise(splits[9], (SFF, D), SFF ** -0.5, 0.25, ((0, 4), (1, 4)), jnp.float32)
    return {"tokens": tokens, "routes": routes, "routing_weight": routing_weight, "norm_gain_vector": norm_gain_vector, "expert_gate": expert_gate, "expert_up": expert_up, "expert_down": expert_down, "shared_gate": shared_gate, "shared_up": shared_up, "shared_down": shared_down}


norm_eps = 1e-06

def block_sums(rows, weight):
    count = rows.shape[0]
    outs = weight.shape[0]
    part = D // N_TP
    left_operand = rows.astype(jnp.float32).reshape(count, N_TP, part)
    right_operand = weight.astype(jnp.float32).reshape(outs, N_TP, part)
    fragments = jnp.einsum('ucb,xcb->cux', left_operand, right_operand)
    rounded = lax.optimization_barrier(fragments.astype(jnp.bfloat16))
    return lax.optimization_barrier(jnp.sum(rounded.astype(jnp.float32), axis=0))

def reference(tokens, routes, routing_weight, norm_gain_vector, expert_gate, expert_up, expert_down, shared_gate, shared_up, shared_down):
    gate_served = (expert_gate * norm_gain_vector[None, None, :]).astype(jnp.bfloat16)
    up_served = (expert_up * norm_gain_vector[None, None, :]).astype(jnp.bfloat16)
    down_served = expert_down.astype(jnp.bfloat16)
    shared_gate_served = (shared_gate * norm_gain_vector[None, :]).astype(jnp.bfloat16)
    shared_up_served = (shared_up * norm_gain_vector[None, :]).astype(jnp.bfloat16)
    shared_down_served = shared_down.astype(jnp.bfloat16)
    values = tokens.astype(jnp.float32)
    squares = lax.optimization_barrier(jnp.sum(values * values, axis=1, keepdims=True))
    normed = (values * lax.rsqrt(squares / D + norm_eps)).astype(jnp.bfloat16)
    grouped = routes.reshape(N_FS, TOK_G * TOPK)
    onehot = (grouped[:, :, None] == jnp.arange(EXPERTS, dtype=jnp.int32)[None, None, :]).astype(jnp.int32)
    earlier = jnp.cumsum(onehot, axis=1) - onehot
    slot_index = lax.optimization_barrier(jnp.sum(earlier * onehot, axis=2))
    blocks = jnp.arange(N_FS, dtype=jnp.int32)[:, None]
    target = (grouped * (N_FS * CAP) + blocks * CAP + slot_index).reshape(-1).astype(jnp.int32)
    token_ids = jnp.repeat(jnp.arange(TOKENS, dtype=jnp.int32), TOPK)
    row_table = jnp.full((EXPERTS * N_FS * CAP,), TOKENS, jnp.int32).at[target].set(token_ids)
    row_table = row_table.reshape(EXPERTS, N_FS * CAP)
    weight_table = jnp.zeros((EXPERTS * N_FS * CAP,), jnp.float32).at[target].set(routing_weight.reshape(-1).astype(jnp.float32))
    weight_table = weight_table.reshape(EXPERTS, N_FS * CAP)
    padded = jnp.concatenate([normed, jnp.zeros((1, D), jnp.bfloat16)], axis=0)

    def one_expert(total, items):
        row_ids, weights, gate_w, up_w, down_w = items
        rows = padded[row_ids]
        hidden = (jax.nn.silu(block_sums(rows, gate_w)) * block_sums(rows, up_w)).astype(jnp.bfloat16)
        produced = jnp.dot(hidden, down_w, preferred_element_type=jnp.float32).astype(jnp.bfloat16)
        return (total.at[row_ids].add(weights[:, None] * produced.astype(jnp.float32)), None)
    routed, _ = lax.scan(one_expert, jnp.zeros((TOKENS + 1, D), jnp.float32), (row_table, weight_table, gate_served, up_served, down_served))
    shared_hidden = (jax.nn.silu(block_sums(normed, shared_gate_served)) * block_sums(normed, shared_up_served)).astype(jnp.bfloat16)
    shared_out = jnp.dot(shared_hidden, shared_down_served, preferred_element_type=jnp.float32)
    mixed = (routed[:TOKENS] + shared_out).astype(jnp.bfloat16)
    return (mixed, gate_served, up_served, down_served, shared_gate_served, shared_up_served, shared_down_served)
```

```python
import functools

import jax
import jax.numpy as jnp
from jax import lax
from jax.experimental import pallas as pl
from jax.experimental.pallas import tpu as pltpu
from jax.sharding import PartitionSpec as P

norm_eps = 1e-06


def dense_rows(rows, weight):
    return lax.dot_general(
        rows, weight, (((1,), (1,)), ((), ())), preferred_element_type=jnp.float32
    )


def per_device_plain(
    tokens,
    routes,
    routing_weight,
    norm_gain_vector,
    expert_gate,
    expert_up,
    expert_down,
    shared_gate,
    shared_up,
    shared_down,
):
    tok_rows, portion_width = tokens.shape
    model_width = portion_width * lax.axis_size("tp")
    experts = expert_gate.shape[0]
    top_count = routes.shape[1]
    capacity = tok_rows * top_count * 7 // (6 * experts)
    gate_round = (expert_gate * norm_gain_vector[None, None, :]).astype(jnp.bfloat16)
    up_round = (expert_up * norm_gain_vector[None, None, :]).astype(jnp.bfloat16)
    down_round = expert_down.astype(jnp.bfloat16)
    gate_refreshed, up_new, down_new = (
        lax.all_to_all(gate_round, "fs", split_axis=0, concat_axis=1, tiled=True),
        lax.all_to_all(up_round, "fs", split_axis=0, concat_axis=1, tiled=True),
        lax.all_to_all(down_round, "fs", split_axis=0, concat_axis=1, tiled=True),
    )
    shared_g, shared_u, shared_d = (
        lax.all_gather(
            (shared_gate * norm_gain_vector[None, :]).astype(jnp.bfloat16), "fs", axis=0, tiled=True
        ),
        lax.all_gather(
            (shared_up * norm_gain_vector[None, :]).astype(jnp.bfloat16), "fs", axis=0, tiled=True
        ),
        lax.all_gather(shared_down.astype(jnp.bfloat16), "fs", axis=0, tiled=True),
    )
    values = tokens.astype(jnp.float32)
    totals = lax.psum(jnp.sum(values * values, axis=1), "tp")
    normed = (values * lax.rsqrt(totals / model_width + norm_eps)[:, None]).astype(jnp.bfloat16)
    flat_expert = routes.reshape(-1)
    onehot = (flat_expert[:, None] == jnp.arange(experts, dtype=jnp.int32)[None, :]).astype(
        jnp.int32
    )
    earlier = jnp.cumsum(onehot, axis=0) - onehot
    slot_index = jnp.sum(earlier * onehot, axis=1)
    target = (flat_expert * capacity + slot_index).reshape(tok_rows, top_count)
    places = jnp.arange(experts * capacity, dtype=jnp.int32)
    placing = jnp.sum(
        (target[:, :, None] == places[None, None, :]).astype(jnp.int32), axis=1
    ).astype(jnp.bfloat16)
    outgoing = lax.dot_general(
        placing, normed, (((0,), (0,)), ((), ())), preferred_element_type=jnp.float32
    ).astype(jnp.bfloat16)
    incoming = lax.all_to_all(
        outgoing.reshape(experts, capacity, portion_width),
        "fs",
        split_axis=0,
        concat_axis=0,
        tiled=True,
    )
    arrived = incoming.reshape(experts * capacity, portion_width)
    partials = (
        dense_rows(arrived, gate_refreshed[0]).astype(jnp.bfloat16),
        dense_rows(arrived, up_new[0]).astype(jnp.bfloat16),
        dense_rows(normed, shared_g).astype(jnp.bfloat16),
        dense_rows(normed, shared_u).astype(jnp.bfloat16),
    )
    gate_part, up_part, sgate_part, sup_part = (
        lax.psum_scatter(partials[0], "tp", scatter_dimension=1, tiled=True).astype(jnp.float32),
        lax.psum_scatter(partials[1], "tp", scatter_dimension=1, tiled=True).astype(jnp.float32),
        lax.psum_scatter(partials[2], "tp", scatter_dimension=1, tiled=True).astype(jnp.float32),
        lax.psum_scatter(partials[3], "tp", scatter_dimension=1, tiled=True).astype(jnp.float32),
    )
    hidden, shared_hidden = (
        lax.all_gather(
            (jax.nn.silu(gate_part) * up_part).astype(jnp.bfloat16), "tp", axis=1, tiled=True
        ),
        lax.all_gather(
            (jax.nn.silu(sgate_part) * sup_part).astype(jnp.bfloat16), "tp", axis=1, tiled=True
        ),
    )
    produced = jnp.dot(hidden, down_new[0], preferred_element_type=jnp.float32).astype(jnp.bfloat16)
    returned = lax.all_to_all(
        produced.reshape(experts, capacity, portion_width),
        "fs",
        split_axis=0,
        concat_axis=0,
        tiled=True,
    )
    picked = returned.reshape(experts * capacity, portion_width)[target]
    routed = jnp.sum(routing_weight[:, :, None] * picked.astype(jnp.float32), axis=1)
    shared_out = jnp.dot(shared_hidden, shared_d, preferred_element_type=jnp.float32)
    mixed = (routed + shared_out).astype(jnp.bfloat16)
    return (mixed, gate_refreshed, up_new, down_new, shared_g, shared_u, shared_d)


MESH = pl.DeviceIdType.MESH


def outward_first(n):
    def key(f):
        return lambda s: (abs(s - f), abs(2 * s - n + 1) <= abs(2 * f - n + 1), s)

    orders = [sorted(range(n), key=key(f)) for f in range(n)]
    return [sum(orders[f][i] * n**f for f in range(n)) for i in range(n)]


def fused_kernel(
    n_fs, n_tp, top_count,
    tok_in, routes_in, weight_in, gain_in, eg_in, eu_in, ed_in, sg_in, su_in, sd_in,
    mixed_ref, wout_ref,
    raw, routes_ref, weight_ref, gain_ref,
    wall, tokbuf, meta_ref, metabuf, ssown, ssbuf, scown, scbuf, mt, sct, part, rsbuf, hid, acc, outb, chain,
    in_s, tok_s, tok_r, meta_s, meta_r, ss_s, ss_r, sc_s, sc_r, rs_s, rs_r, ag_s, ag_r,
    ch_s, ch_r, we_s, we_r, ws_s, ws_r, yw_s, yw_r,
):
    g, f, t = lax.axis_index("grp"), lax.axis_index("fs"), lax.axis_index("tp")
    _, _, rows, width = (n_fs, 2, 2 * tokbuf.shape[2], tokbuf.shape[3])
    experts, units = eg_in.shape[0], eg_in.shape[1]
    sub = rows // n_tp
    half, mid_row = units // 2, rows // 2
    f32, bf16 = jnp.float32, jnp.bfloat16
    code = outward_first(n_fs)
    scope = jax.named_scope

    def source(i):
        total = 0
        digits = code[i]
        picks = [(digits // n_fs**q) % n_fs for q in range(n_fs)]
        for q in range(n_fs):
            hit = 1 - jnp.minimum(1, jnp.abs(f - q))
            total = total + picks[q] * hit
        return total

    at_edge = (f == 0) | (f == n_fs - 1)
    inside = (f > 0) & (f < n_fs - 1)

    def at_fs(index):
        return (g, index, t)

    def at_tp(index):
        return (g, f, index)

    partner = (1 - g, f, t)

    def remote(src, dst, send, recv, device):
        return pltpu.make_async_remote_copy(
            src_ref=src, dst_ref=dst, send_sem=send, recv_sem=recv,
            device_id=device, device_id_type=MESH,
        )

    fs_others = [lax.rem(f + j, n_fs) for j in range(1, n_fs)]
    tp_others = [lax.rem(t + j, n_tp) for j in range(1, n_tp)]

    barrier = pltpu.get_barrier_semaphore()
    peers = [at_fs(d) for d in fs_others] + [at_tp(d) for d in tp_others] + [partner]
    for device in peers:
        pl.semaphore_signal(barrier, inc=1, device_id=device, device_id_type=MESH)

    loads = [pltpu.make_async_copy(tok_in.at[pl.ds(h * mid_row, mid_row)], tokbuf.at[f, h], in_s.at[h]) for h in range(2)]
    loads.append(pltpu.make_async_copy(routes_in, routes_ref, in_s.at[2]))
    loads.append(pltpu.make_async_copy(weight_in, weight_ref, in_s.at[3]))
    loads.append(pltpu.make_async_copy(gain_in, gain_ref, in_s.at[4]))
    for m, (routed, shared) in enumerate(((eg_in, sg_in), (eu_in, su_in), (ed_in, sd_in))):
        loads.append(pltpu.make_async_copy(routed, raw.at[m, pl.ds(0, experts)], in_s.at[5 + 2 * m]))
        loads.append(pltpu.make_async_copy(shared, raw.at[m, experts], in_s.at[6 + 2 * m]))
    for load in loads:
        load.start()
    for load in loads[:4]:
        load.wait()
    meta_ref[...] = jnp.zeros(meta_ref.shape, f32)
    meta_ref[0:top_count, 0:rows] = routes_ref[...].astype(f32)
    meta_ref[top_count : 2 * top_count, 0:rows] = weight_ref[...]

    def own_tokens():
        return tokbuf[f].reshape(rows, width)

    x = own_tokens().astype(f32)
    sq = x * x
    high = sq.astype(bf16)
    low = (sq - high.astype(f32)).astype(bf16)
    ones = jnp.ones((8, width), bf16)
    ssown[...] = jnp.zeros(ssown.shape, f32)
    ssown[:, 0:rows] = dense_rows(ones, high) + dense_rows(ones, low)

    with scope("barrier"):
        pl.semaphore_wait(barrier, len(peers))

    def to_right(src, dst, send, recv):
        @pl.when(f < n_fs - 1)
        def _():
            remote(src, dst, send, recv, at_fs(f + 1)).start()

    def to_left(src, dst, send, recv):
        @pl.when(f > 0)
        def _():
            remote(src, dst, send, recv, at_fs(f - 1)).start()

    def onward(s, ref, send, recv):
        @pl.when((s < f) & (f < n_fs - 1))
        def _():
            remote(ref, ref, send(0), recv, at_fs(f + 1)).start()

        @pl.when((s > f) & (f > 0))
        def _():
            remote(ref, ref, send(1), recv, at_fs(f - 1)).start()

    def line_sends_done(refs, send, recv):
        for s in range(n_fs):
            ref = refs(s)

            @pl.when((f >= s) & (f < n_fs - 1))
            def _():
                remote(ref, ref, send(s, 0), recv(s), at_fs(f + 1)).wait_send()

            @pl.when((f <= s) & (f > 0))
            def _():
                remote(ref, ref, send(s, 1), recv(s), at_fs(f - 1)).wait_send()

    for way, go in ((0, to_right), (1, to_left)):
        go(meta_ref, metabuf.at[f], meta_s.at[f, way], meta_r.at[f])
        for h in range(2):
            go(tokbuf.at[f, h], tokbuf.at[f, h], tok_s.at[f, way, h], tok_r.at[f, h])
    for d in tp_others:
        remote(ssown, ssbuf.at[t], ss_s.at[d], ss_r.at[t], at_tp(d)).start()

    def convert(m):
        for load in loads[5 + 2 * m : 7 + 2 * m]:
            load.wait()
        for e in range(experts + 1):
            value = raw[m, e]
            wall[m, e] = (value * gain_ref[...] if m < 2 else value).astype(bf16)

    def transposed(row_ref):
        return jnp.transpose(row_ref[...])[0:rows]

    def forward_block(i, s, meta):
        mt[i] = transposed(meta)
        tokens = tokbuf[s].reshape(rows, width)
        names = [mt[i, :, k : k + 1] for k in range(top_count)]
        columns = []
        for m in range(2):
            weight = wall[m].reshape((experts + 1) * units, width)
            sums = dense_rows(tokens, weight)
            for name in names:
                chosen = jnp.zeros((rows, units), f32)
                for e in range(experts):
                    chosen = jnp.where(name == float(e), sums[:, e * units : (e + 1) * units], chosen)
                columns.append(chosen)
            columns.append(sums[:, experts * units :])
        for c, column in enumerate(columns):
            part[i, :, :, c * units : (c + 1) * units] = column.astype(bf16).reshape(n_tp, sub, units)
        for d in tp_others:
            remote(part.at[i, d], rsbuf.at[i, t], rs_s.at[i, d], rs_r.at[i, t], at_tp(d)).start()

    def hidden_block(i, scale_row):
        sct[i] = transposed(scale_row)
        own_rows = pl.ds(pl.multiple_of(t * sub, 8), sub)
        scale = sct[i, own_rows, 0:1]
        weights = mt[i, own_rows, :]
        for d in tp_others:
            remote(part.at[i, d], rsbuf.at[i, d], rs_s.at[i, d], rs_r.at[i, d], at_tp(d)).wait_recv()
        total = part[i, t].astype(f32)
        for d in tp_others:
            total = total + rsbuf[i, d].astype(f32)
        total = total * scale
        kinds = top_count + 1
        for k in range(kinds):
            gate = total[:, k * units : (k + 1) * units]
            up = total[:, (kinds + k) * units : (kinds + k + 1) * units]
            value = jax.nn.silu(gate) * up
            if k < top_count:
                value = value * weights[:, top_count + k : top_count + k + 1]
            hid[i, t, :, k * units : (k + 1) * units] = value.astype(bf16)
        for d in tp_others:
            remote(hid.at[i, t], hid.at[i, t], ag_s.at[i, d], ag_r.at[i, t], at_tp(d)).start()

    def down_block(i):
        for d in tp_others:
            remote(hid.at[i, d], hid.at[i, d], ag_s.at[i, d], ag_r.at[i, d], at_tp(d)).wait_recv()
        values = hid[i].astype(f32).reshape(rows, (top_count + 1) * units)
        names = [mt[i, :, k : k + 1] for k in range(top_count)]
        spread = []
        for e in range(experts):
            chosen = jnp.zeros((rows, units), f32)
            for k, name in enumerate(names):
                chosen = jnp.where(name == float(e), values[:, k * units : (k + 1) * units], chosen)
            spread.append(chosen.astype(bf16))
        spread.append(values[:, top_count * units :].astype(bf16))
        weight = wall[2].reshape((experts + 1) * units, width)
        product = jnp.dot(jnp.concatenate(spread, axis=1), weight, preferred_element_type=f32)
        acc[i] = product.reshape(2, mid_row, width)

    def chain_send(i, h):
        d = source(i)

        @pl.when(d > f)
        def _():
            remote(outb.at[i, h], chain.at[d, h], ch_s.at[i, h], ch_r.at[d, h], at_fs(f + 1)).start()

        @pl.when(d < f)
        def _():
            slot = d + (n_fs - d) * (1 - jnp.minimum(1, f - 1 - d))
            remote(outb.at[i, h], chain.at[slot, h], ch_s.at[i, h], ch_r.at[slot, h], at_fs(f - 1)).start()

    def finish_block(i):
        with scope(f"down{i}"):
            down_block(i)
        if i > 0:

            @pl.when(at_edge)
            def _():
                for h in range(2):
                    outb[i, h] = acc[i, h].astype(bf16)
                    chain_send(i, h)

    def chain_wait(slot, h):
        remote(chain.at[slot, h], chain.at[slot, h], ch_s.at[1, h], ch_r.at[slot, h], partner).wait_recv()

    def chain_on(i):
        @pl.when(inside)
        def _():
            d = source(i)
            for h in range(2):
                with scope(f"chain{i}{h}"):
                    chain_wait(d, h)
                outb[i, h] = (acc[i, h] + chain[d, h].astype(f32)).astype(bf16)
                chain_send(i, h)

    def token_block(i):
        s = source(i)
        with scope(f"tok{i}"):
            remote(metabuf.at[s], metabuf.at[s], meta_s.at[s, 0], meta_r.at[s], partner).wait_recv()
            onward(s, metabuf.at[s], lambda way: meta_s.at[s, way], meta_r.at[s])
            for h in range(2):
                remote(tokbuf.at[s, h], tokbuf.at[s, h], tok_s.at[s, 0, h], tok_r.at[s, h], partner).wait_recv()
                onward(s, tokbuf.at[s, h], lambda way: tok_s.at[s, way, h], tok_r.at[s, h])

    def scale_block(i):
        s = source(i)
        remote(scown, scbuf.at[s], sc_s.at[s], sc_r.at[s], partner).wait_recv()
        return scbuf.at[s]

    mine = pl.ds(pl.multiple_of(g * half, 16), half)

    def give_shared(i):
        d = source(i)
        for m in range(3):
            src, dst = wall.at[m, experts, mine], wout_ref.at[1, m, f, g]

            @pl.when(d == f + 1)
            def _():
                remote(src, dst, ws_s.at[f, 0, m], ws_r.at[f, m], at_fs(f + 1)).start()

            @pl.when(d == f - 1)
            def _():
                remote(src, dst, ws_s.at[f, 1, m], ws_r.at[f, m], at_fs(f - 1)).start()

    def give_expert(i):
        d = source(i)
        for m in range(3):
            remote(
                wall.at[m, d, mine], wout_ref.at[0, m, f, g], we_s.at[i, m], we_r.at[f, m], at_fs(d)
            ).start()

    def pass_shared(i):
        s = source(i)
        for m in range(3):
            ref = wout_ref.at[1, m, s, g]
            with scope(f"S{i}{m}"):
                remote(ref, ref, ws_s.at[s, 0, m], ws_r.at[s, m], partner).wait_recv()
            onward(s, ref, lambda way: ws_s.at[s, way, m], ws_r.at[s, m])
            remote(ref, ref, yw_s.at[1, s, m], yw_r.at[1, s, m], partner).start()

    def pass_routed(i):
        s = source(i)
        for m in range(3):
            ref = wout_ref.at[0, m, s, g]
            with scope(f"E{i}{m}"):
                remote(ref, ref, we_s.at[i, m], we_r.at[s, m], partner).wait_recv()
            remote(ref, ref, yw_s.at[0, s, m], yw_r.at[0, s, m], partner).start()

    loads[4].wait()
    convert(0)
    convert(1)
    forward_block(0, f, meta_ref)
    squares = ssown[...]
    with scope("sswait"):
        for d in tp_others:
            remote(ssown, ssbuf.at[d], ss_s.at[d], ss_r.at[d], at_tp(d)).wait_recv()
            squares = squares + ssbuf[d]
    scown[...] = lax.rsqrt(squares / (width * n_tp) + norm_eps)
    for d in fs_others:
        remote(scown, scbuf.at[f], sc_s.at[d], sc_r.at[f], at_fs(d)).start()
    convert(2)

    @pl.when(at_edge)
    def _():
        give_shared(1)
        for i in range(1, n_fs):
            give_expert(i)

    for h in range(2):
        wout_ref[0, :, f, h] = wall[:, f, h * half : (h + 1) * half]
        wout_ref[1, :, f, h] = wall[:, experts, h * half : (h + 1) * half]

    def arrive(i):
        token_block(i)

        if i == 1:

            @pl.when(inside)
            def _():
                give_shared(2)
                give_expert(2)

        if i == n_fs - 1:

            @pl.when(inside)
            def _():
                give_shared(1)
                give_expert(1)

        with scope(f"fwd{i}"):
            forward_block(i, source(i), metabuf.at[source(i)])

    def hide(i):
        with scope(f"hid{i}"):
            hidden_block(i, scown if i == 0 else scale_block(i))

    arrive(1)
    arrive(2)
    hide(0)
    arrive(3)
    hide(1)
    hide(2)
    finish_block(0)
    finish_block(1)
    pass_shared(1)

    @pl.when(inside)
    def _():
        give_expert(n_fs - 1)

    hide(3)
    finish_block(2)

    @pl.when(inside)
    def _():
        pass_shared(2)

    finish_block(3)
    pass_routed(1)

    @pl.when(at_edge)
    def _():
        pass_shared(2)

    pass_routed(2)
    pass_shared(3)
    chain_on(2)
    pass_routed(3)
    chain_on(3)
    chain_on(1)

    for h in range(2):
        with scope(f"last{h}"):

            @pl.when(f > 0)
            def _():
                chain_wait(f, h)
                acc[0, h] = acc[0, h] + chain[f, h].astype(f32)

            @pl.when(f < n_fs - 1)
            def _():
                chain_wait(n_fs, h)
                acc[0, h] = acc[0, h] + chain[n_fs, h].astype(f32)

        mixed_ref[h * mid_row : (h + 1) * mid_row] = acc[0, h].astype(bf16)

    with scope("ywait"):
        for d in fs_others:
            for kind in range(2):
                for m in range(3):
                    ref = wout_ref.at[kind, m, d, 1 - g]
                    remote(ref, ref, yw_s.at[kind, d, m], yw_r.at[kind, d, m], partner).wait_recv()

    with scope("drain"):
        line_sends_done(lambda s: metabuf.at[s], lambda s, way: meta_s.at[s, way], lambda s: meta_r.at[s])
        for h in range(2):
            line_sends_done(lambda s: tokbuf.at[s, h], lambda s, way: tok_s.at[s, way, h], lambda s: tok_r.at[s, h])
        for m in range(3):
            line_sends_done(
                lambda s: wout_ref.at[1, m, s, g], lambda s, way: ws_s.at[s, way, m], lambda s: ws_r.at[s, m]
            )
        for d in tp_others:
            remote(ssown, ssbuf.at[t], ss_s.at[d], ss_r.at[t], at_tp(d)).wait_send()
            for i in range(n_fs):
                remote(part.at[i, d], rsbuf.at[i, t], rs_s.at[i, d], rs_r.at[i, t], at_tp(d)).wait_send()
                remote(hid.at[i, t], hid.at[i, t], ag_s.at[i, d], ag_r.at[i, t], at_tp(d)).wait_send()
        for d in fs_others:
            remote(scown, scbuf.at[f], sc_s.at[d], sc_r.at[f], at_fs(d)).wait_send()
        for i in range(1, n_fs):
            s = source(i)
            for h in range(2):
                remote(outb.at[i, h], chain.at[f, h], ch_s.at[i, h], ch_r.at[f, h], partner).wait_send()
            for m in range(3):
                routed, shared = wout_ref.at[0, m, s, g], wout_ref.at[1, m, s, g]
                remote(routed, routed, we_s.at[i, m], we_r.at[f, m], partner).wait_send()
                remote(routed, routed, yw_s.at[0, s, m], yw_r.at[0, s, m], partner).wait_send()
                remote(shared, shared, yw_s.at[1, s, m], yw_r.at[1, s, m], partner).wait_send()


def put_out(mixed_ref, served_ref, *rest):
    outs, sems = rest[:-1], rest[-1]
    copies = [pltpu.make_async_copy(served_ref.at[i], outs[1 + i], sems.at[1 + i]) for i in range(len(outs) - 1)]
    copies.append(pltpu.make_async_copy(mixed_ref, outs[0], sems.at[0]))
    for copy in copies:
        copy.start()
    for copy in copies:
        copy.wait()


def per_device_fused(
    tokens,
    routes,
    routing_weight,
    norm_gain_vector,
    expert_gate,
    expert_up,
    expert_down,
    shared_gate,
    shared_up,
    shared_down,
):
    n_fs, n_tp = lax.axis_size("fs"), lax.axis_size("tp")
    rows, width = tokens.shape
    experts, units, _ = expert_gate.shape
    top_count = routes.shape[1]
    sub, half = rows // n_tp, units // 2
    meta_rows = -(-2 * top_count // 8) * 8
    lanes = -(-rows // 128) * 128
    f32, bf16 = jnp.float32, jnp.bfloat16
    kinds = top_count + 1
    dma = pltpu.SemaphoreType.DMA
    vmem = pl.BlockSpec(memory_space=pltpu.VMEM)
    hbm = pl.BlockSpec(memory_space=pltpu.HBM)
    mixed, served = pl.pallas_call(
        functools.partial(fused_kernel, n_fs, n_tp, top_count),
        out_shape=(
            pltpu.VMEM((rows, width), bf16),
            pltpu.VMEM((2, 3, n_fs, 2, half, width), bf16),
        ),
        in_specs=[hbm] * 10,
        out_specs=(vmem, vmem),
        scratch_shapes=[
            pltpu.VMEM((3, experts + 1, units, width), f32),
            pltpu.VMEM((top_count, rows), jnp.int32),
            pltpu.VMEM((top_count, rows), f32),
            pltpu.VMEM((1, width), f32),
            pltpu.VMEM((3, experts + 1, units, width), bf16),
            pltpu.VMEM((n_fs, 2, rows // 2, width), bf16),
            pltpu.VMEM((meta_rows, lanes), f32),
            pltpu.VMEM((n_fs, meta_rows, lanes), f32),
            pltpu.VMEM((8, lanes), f32),
            pltpu.VMEM((n_tp, 8, lanes), f32),
            pltpu.VMEM((8, lanes), f32),
            pltpu.VMEM((n_fs, 8, lanes), f32),
            pltpu.VMEM((n_fs, rows, meta_rows), f32),
            pltpu.VMEM((n_fs, rows, 8), f32),
            pltpu.VMEM((n_fs, n_tp, sub, 2 * kinds * units), bf16),
            pltpu.VMEM((n_fs, n_tp, sub, 2 * kinds * units), bf16),
            pltpu.VMEM((n_fs, n_tp, sub, kinds * units), bf16),
            pltpu.VMEM((n_fs, 2, rows // 2, width), f32),
            pltpu.VMEM((n_fs, 2, rows // 2, width), bf16),
            pltpu.VMEM((n_fs + 1, 2, rows // 2, width), bf16),
            dma((11,)),
            dma((n_fs, 2, 2)), dma((n_fs, 2)),
            dma((n_fs, 2)), dma((n_fs,)),
            dma((n_tp,)), dma((n_tp,)),
            dma((n_fs,)), dma((n_fs,)),
            dma((n_fs, n_tp)), dma((n_fs, n_tp)),
            dma((n_fs, n_tp)), dma((n_fs, n_tp)),
            dma((n_fs, 2)), dma((n_fs + 1, 2)),
            dma((n_fs, 3)), dma((n_fs, 3)),
            dma((n_fs, 2, 3)), dma((n_fs, 3)),
            dma((2, n_fs, 3)), dma((2, n_fs, 3)),
        ],
        compiler_params=pltpu.CompilerParams(
            collective_id=0, has_side_effects=True, vmem_limit_bytes=40 * 1024 * 1024
        ),
        name="hand_over_and_layer",
    )(*[
        pltpu.with_memory_space_constraint(value, pltpu.HBM)
        for value in (
            tokens, routes.T, routing_weight.T, norm_gain_vector[None, :],
            expert_gate, expert_up, expert_down, shared_gate, shared_up, shared_down,
        )
    ])
    units_all = n_fs * units
    outs = pl.pallas_call(
        put_out,
        out_shape=(
            jax.ShapeDtypeStruct((rows, width), bf16),
            *[jax.ShapeDtypeStruct((units_all, width), bf16)] * 6,
        ),
        in_specs=[vmem] * 2,
        out_specs=(hbm,) * 7,
        scratch_shapes=[dma((7,))],
        compiler_params=pltpu.CompilerParams(vmem_limit_bytes=8 * 1024 * 1024),
        name="put_out",
    )(mixed, served.reshape(6, units_all, width))
    return (outs[0], outs[1][None], outs[2][None], outs[3][None], *outs[4:])


def per_device(tokens, routes, routing_weight, norm_gain_vector, *weights):
    experts, units, width = weights[0].shape
    rows, n_fs, n_tp = tokens.shape[0], lax.axis_size("fs"), lax.axis_size("tp")
    whole_tiles = units % 128 == 0 and width % 128 == 0 and rows % (16 * n_tp) == 0
    fits = (experts + 1) * units * width <= 2**20 and n_fs == 4 and n_tp <= 4
    chosen = per_device_plain
    if whole_tiles and fits and experts == n_fs and lax.axis_size("grp") == 2:
        chosen = per_device_fused
    return chosen(tokens, routes, routing_weight, norm_gain_vector, *weights)


def solution(mesh):
    return jax.shard_map(
        per_device,
        mesh=mesh,
        in_specs=(
            P(("grp", "fs"), "tp"),
            P(("grp", "fs"), None),
            P(("grp", "fs"), None),
            P("tp"),
            P(None, "fs", "tp"),
            P(None, "fs", "tp"),
            P(None, "fs", "tp"),
            P("fs", "tp"),
            P("fs", "tp"),
            P("fs", "tp"),
        ),
        out_specs=(
            P(("grp", "fs"), "tp"),
            P(("grp", "fs"), None, "tp"),
            P(("grp", "fs"), None, "tp"),
            P(("grp", "fs"), None, "tp"),
            P("grp", "tp"),
            P("grp", "tp"),
            P("grp", "tp"),
        ),
        check_vma=False,
    )
```

```python
import functools

import jax
import jax.numpy as jnp
from jax import lax
from jax.experimental import pallas as pl
from jax.experimental.pallas import tpu as pltpu
from jax.sharding import PartitionSpec as P

norm_eps = 1e-06


def dense_rows(rows, weight):
    return lax.dot_general(
        rows, weight, (((1,), (1,)), ((), ())), preferred_element_type=jnp.float32
    )


def per_device_plain(
    tokens,
    routes,
    routing_weight,
    norm_gain_vector,
    expert_gate,
    expert_up,
    expert_down,
    shared_gate,
    shared_up,
    shared_down,
):
    tok_rows, portion_width = tokens.shape
    model_width = portion_width * lax.axis_size("tp")
    experts = expert_gate.shape[0]
    top_count = routes.shape[1]
    capacity = tok_rows * top_count * 7 // (6 * experts)
    gate_round = (expert_gate * norm_gain_vector[None, None, :]).astype(jnp.bfloat16)
    up_round = (expert_up * norm_gain_vector[None, None, :]).astype(jnp.bfloat16)
    down_round = expert_down.astype(jnp.bfloat16)
    gate_refreshed, up_new, down_new = (
        lax.all_to_all(gate_round, "fs", split_axis=0, concat_axis=1, tiled=True),
        lax.all_to_all(up_round, "fs", split_axis=0, concat_axis=1, tiled=True),
        lax.all_to_all(down_round, "fs", split_axis=0, concat_axis=1, tiled=True),
    )
    shared_g, shared_u, shared_d = (
        lax.all_gather(
            (shared_gate * norm_gain_vector[None, :]).astype(jnp.bfloat16), "fs", axis=0, tiled=True
        ),
        lax.all_gather(
            (shared_up * norm_gain_vector[None, :]).astype(jnp.bfloat16), "fs", axis=0, tiled=True
        ),
        lax.all_gather(shared_down.astype(jnp.bfloat16), "fs", axis=0, tiled=True),
    )
    values = tokens.astype(jnp.float32)
    totals = lax.psum(jnp.sum(values * values, axis=1), "tp")
    normed = (values * lax.rsqrt(totals / model_width + norm_eps)[:, None]).astype(jnp.bfloat16)
    flat_expert = routes.reshape(-1)
    onehot = (flat_expert[:, None] == jnp.arange(experts, dtype=jnp.int32)[None, :]).astype(
        jnp.int32
    )
    earlier = jnp.cumsum(onehot, axis=0) - onehot
    slot_index = jnp.sum(earlier * onehot, axis=1)
    target = (flat_expert * capacity + slot_index).reshape(tok_rows, top_count)
    places = jnp.arange(experts * capacity, dtype=jnp.int32)
    placing = jnp.sum(
        (target[:, :, None] == places[None, None, :]).astype(jnp.int32), axis=1
    ).astype(jnp.bfloat16)
    outgoing = lax.dot_general(
        placing, normed, (((0,), (0,)), ((), ())), preferred_element_type=jnp.float32
    ).astype(jnp.bfloat16)
    incoming = lax.all_to_all(
        outgoing.reshape(experts, capacity, portion_width),
        "fs",
        split_axis=0,
        concat_axis=0,
        tiled=True,
    )
    arrived = incoming.reshape(experts * capacity, portion_width)
    partials = (
        dense_rows(arrived, gate_refreshed[0]).astype(jnp.bfloat16),
        dense_rows(arrived, up_new[0]).astype(jnp.bfloat16),
        dense_rows(normed, shared_g).astype(jnp.bfloat16),
        dense_rows(normed, shared_u).astype(jnp.bfloat16),
    )
    gate_part, up_part, sgate_part, sup_part = (
        lax.psum_scatter(partials[0], "tp", scatter_dimension=1, tiled=True).astype(jnp.float32),
        lax.psum_scatter(partials[1], "tp", scatter_dimension=1, tiled=True).astype(jnp.float32),
        lax.psum_scatter(partials[2], "tp", scatter_dimension=1, tiled=True).astype(jnp.float32),
        lax.psum_scatter(partials[3], "tp", scatter_dimension=1, tiled=True).astype(jnp.float32),
    )
    hidden, shared_hidden = (
        lax.all_gather(
            (jax.nn.silu(gate_part) * up_part).astype(jnp.bfloat16), "tp", axis=1, tiled=True
        ),
        lax.all_gather(
            (jax.nn.silu(sgate_part) * sup_part).astype(jnp.bfloat16), "tp", axis=1, tiled=True
        ),
    )
    produced = jnp.dot(hidden, down_new[0], preferred_element_type=jnp.float32).astype(jnp.bfloat16)
    returned = lax.all_to_all(
        produced.reshape(experts, capacity, portion_width),
        "fs",
        split_axis=0,
        concat_axis=0,
        tiled=True,
    )
    picked = returned.reshape(experts * capacity, portion_width)[target]
    routed = jnp.sum(routing_weight[:, :, None] * picked.astype(jnp.float32), axis=1)
    shared_out = jnp.dot(shared_hidden, shared_d, preferred_element_type=jnp.float32)
    mixed = (routed + shared_out).astype(jnp.bfloat16)
    return (mixed, gate_refreshed, up_new, down_new, shared_g, shared_u, shared_d)


MESH = pl.DeviceIdType.MESH


def outward_first(n):
    def key(f):
        return lambda s: (abs(s - f), abs(2 * s - n + 1) <= abs(2 * f - n + 1), s)

    orders = [sorted(range(n), key=key(f)) for f in range(n)]
    return [sum(orders[f][i] * n**f for f in range(n)) for i in range(n)]


def fused_kernel(
    n_fs, n_tp, top_count,
    tok_in, routes_in, weight_in, gain_in, eg_in, eu_in, ed_in, sg_in, su_in, sd_in,
    mixed_ref, wout_ref,
    raw, routes_ref, weight_ref, gain_ref,
    wall, tokbuf, meta_ref, metabuf, ssown, ssbuf, scown, scbuf, mt, sct, part, rsbuf, hid, acc, outb, chain,
    in_s, tok_s, tok_r, meta_s, meta_r, ss_s, ss_r, sc_s, sc_r, rs_s, rs_r, ag_s, ag_r,
    ch_s, ch_r, we_s, we_r, ws_s, ws_r, yw_s, yw_r,
):
    g, f, t = lax.axis_index("grp"), lax.axis_index("fs"), lax.axis_index("tp")
    rows, width = tokbuf.shape[1:]
    experts, units = eg_in.shape[0], eg_in.shape[1]
    sub = rows // n_tp
    half = units // 2
    f32, bf16 = jnp.float32, jnp.bfloat16
    code = outward_first(n_fs)
    scope = jax.named_scope
    parts = [pl.ds(h * (rows // 2), rows // 2) for h in range(2)]
    three = pl.ds(0, n_tp - 1)

    def source(i):
        total = 0
        digits = code[i]
        picks = [(digits // n_fs**q) % n_fs for q in range(n_fs)]
        for q in range(n_fs):
            hit = 1 - jnp.minimum(1, jnp.abs(f - q))
            total = total + picks[q] * hit
        return total

    at_edge = (f == 0) | (f == n_fs - 1)
    inside = (f > 0) & (f < n_fs - 1)

    def at_fs(index):
        return (g, index, t)

    def at_tp(index):
        return (g, f, index)

    partner = (1 - g, f, t)

    def remote(src, dst, send, recv, device):
        return pltpu.make_async_remote_copy(
            src_ref=src, dst_ref=dst, send_sem=send, recv_sem=recv,
            device_id=device, device_id_type=MESH,
        )

    def sent(ref, send):
        remote(ref, ref, send, send, partner).wait_send()

    def landed(ref, recv):
        remote(ref, ref, recv, recv, partner).wait_recv()

    fs_others = [lax.rem(f + j, n_fs) for j in range(1, n_fs)]
    tp_others = [lax.rem(t + j, n_tp) for j in range(1, n_tp)]

    barrier = pltpu.get_barrier_semaphore()
    peers = [at_fs(d) for d in fs_others] + [at_tp(d) for d in tp_others] + [partner]
    for device in peers:
        pl.semaphore_signal(barrier, inc=1, device_id=device, device_id_type=MESH)

    small = [
        pltpu.make_async_copy(tok_in, tokbuf.at[f], in_s.at[0]),
        pltpu.make_async_copy(routes_in, routes_ref, in_s.at[1]),
        pltpu.make_async_copy(weight_in, weight_ref, in_s.at[2]),
        pltpu.make_async_copy(gain_in, gain_ref, in_s.at[3]),
    ]
    for load in small:
        load.start()
    for m, (routed, shared) in enumerate(((eg_in, sg_in), (eu_in, su_in), (ed_in, sd_in))):
        pltpu.make_async_copy(routed, raw.at[m, pl.ds(0, experts)], in_s.at[4 + m]).start()
        pltpu.make_async_copy(shared, raw.at[m, experts], in_s.at[4 + m]).start()
    for load in small:
        load.wait()
    meta_ref[...] = jnp.zeros(meta_ref.shape, f32)
    meta_ref[0:top_count, 0:rows] = routes_ref[...].astype(f32)
    meta_ref[top_count : 2 * top_count, 0:rows] = weight_ref[...]

    x = tokbuf[f].astype(f32)
    sq = x * x
    high = sq.astype(bf16)
    low = (sq - high.astype(f32)).astype(bf16)
    ones = jnp.ones((8, width), bf16)
    ssown[...] = jnp.zeros(ssown.shape, f32)
    ssown[:, 0:rows] = dense_rows(ones, high) + dense_rows(ones, low)

    with scope("barrier"):
        pl.semaphore_wait(barrier, len(peers))

    def convert(m):
        pltpu.make_async_copy(raw.at[m], raw.at[m], in_s.at[4 + m]).wait()
        for e in range(experts + 1):
            value = raw[m, e]
            wall[m, e] = (value * gain_ref[...] if m < 2 else value).astype(bf16)

    def transposed(row_ref):
        return jnp.transpose(row_ref[...])[0:rows]

    def forward_block(i):
        s = source(i)
        with scope(f"fwd{i}"):
            mt[i] = transposed(meta_ref if i == 0 else metabuf.at[s])
            tokens = tokbuf[s]
            names = [mt[i, :, k : k + 1] for k in range(top_count)]
            columns = []
            for m in range(2):
                weight = wall[m].reshape((experts + 1) * units, width)
                sums = dense_rows(tokens, weight)
                for name in names:
                    chosen = jnp.zeros((rows, units), f32)
                    for e in range(experts):
                        chosen = jnp.where(name == float(e), sums[:, e * units : (e + 1) * units], chosen)
                    columns.append(chosen)
                columns.append(sums[:, experts * units :])
            for c, column in enumerate(columns):
                part[i, :, :, c * units : (c + 1) * units] = column.astype(bf16).reshape(n_tp, sub, units)
            for d in tp_others:
                remote(part.at[i, d], rsbuf.at[i, t], rs_s.at[0], rs_r.at[i], at_tp(d)).start()

    def hidden_block(i):
        s = source(i)
        with scope(f"hid{i}"):
            if i > 0:
                landed(scbuf.at[s], sc_r.at[s])
            sct[i] = transposed(scown if i == 0 else scbuf.at[s])
            own_rows = pl.ds(pl.multiple_of(t * sub, 8), sub)
            scale = sct[i, own_rows, 0:1]
            weights = mt[i, own_rows, :]
            landed(rsbuf.at[i, three], rs_r.at[i])
            total = part[i, t].astype(f32)
            for d in tp_others:
                total = total + rsbuf[i, d].astype(f32)
            total = total * scale
            kinds = top_count + 1
            for k in range(kinds):
                gate = total[:, k * units : (k + 1) * units]
                up = total[:, (kinds + k) * units : (kinds + k + 1) * units]
                value = jax.nn.silu(gate) * up
                if k < top_count:
                    value = value * weights[:, top_count + k : top_count + k + 1]
                hid[i, t, :, k * units : (k + 1) * units] = value.astype(bf16)
            for d in tp_others:
                remote(hid.at[i, t], hid.at[i, t], ag_s.at[0], ag_r.at[i], at_tp(d)).start()

    def down_block(i):
        with scope(f"down{i}"):
            landed(hid.at[i, three], ag_r.at[i])
            values = hid[i].astype(f32).reshape(rows, (top_count + 1) * units)
            names = [mt[i, :, k : k + 1] for k in range(top_count)]
            spread = []
            for e in range(experts):
                chosen = jnp.zeros((rows, units), f32)
                for k, name in enumerate(names):
                    chosen = jnp.where(name == float(e), values[:, k * units : (k + 1) * units], chosen)
                spread.append(chosen.astype(bf16))
            spread.append(values[:, top_count * units :].astype(bf16))
            weight = wall[2].reshape((experts + 1) * units, width)
            acc[i] = jnp.dot(jnp.concatenate(spread, axis=1), weight, preferred_element_type=f32)

    def chain_send(i, h, hop, last):
        d = source(i)
        slot = d
        if last:
            slot = d + (n_fs - d) * jnp.minimum(1, jnp.maximum(0, f - d))
        remote(
            outb.at[i, parts[h]], chain.at[slot, parts[h]], ch_s.at[0], ch_r.at[slot, h], at_fs(source(hop))
        ).start()

    def chain_start(i):
        for h in range(2):
            outb[i, parts[h]] = acc[i, parts[h]].astype(bf16)
            chain_send(i, h, 1, i == 1)

    def chain_on(i, h):
        d = source(i)
        with scope(f"chain{i}{h}"):
            landed(chain.at[d, parts[h]], ch_r.at[d, h])
        outb[i, parts[h]] = (acc[i, parts[h]] + chain[d, parts[h]].astype(f32)).astype(bf16)
        chain_send(i, h, min(i, 2), i < 3)

    def chain_end(slot, h):
        with scope(f"last{h}"):
            landed(chain.at[slot, parts[h]], ch_r.at[slot, h])
        acc[0, parts[h]] = acc[0, parts[h]] + chain[slot, parts[h]].astype(f32)

    def tokens_to(hop, s, h):
        ref = tokbuf.at[s, parts[h]]
        remote(ref, ref, tok_s.at[0], tok_r.at[s, h], at_fs(source(hop))).start()

    def meta_to(hop, s):
        remote(
            meta_ref if s is f else metabuf.at[s], metabuf.at[s], meta_s.at[0], meta_r.at[s], at_fs(source(hop))
        ).start()

    def take_tokens(i, h, hop=None):
        s = source(i)
        with scope(f"tok{i}{h}"):
            if h == 0:
                landed(metabuf.at[s], meta_r.at[s])
                if hop:
                    meta_to(hop, s)
            landed(tokbuf.at[s, parts[h]], tok_r.at[s, h])
            if hop:
                tokens_to(hop, s, h)

    mine = pl.ds(pl.multiple_of(g * half, 16), half)

    def give_shared(hop, pieces=(0, 1, 2)):
        for m in pieces:
            remote(
                wall.at[m, experts, mine], wout_ref.at[1, m, f, g], ws_s.at[0], ws_r.at[f, m], at_fs(source(hop))
            ).start()

    def give_expert(i):
        d = source(i)
        for m in range(3):
            remote(wall.at[m, d, mine], wout_ref.at[0, m, f, g], we_s.at[0], we_r.at[f, m], at_fs(d)).start()

    def pass_shared(i, m, hop=None):
        s = source(i)
        ref = wout_ref.at[1, m, s, g]
        with scope(f"S{i}{m}"):
            landed(ref, ws_r.at[s, m])
        if hop:
            remote(ref, ref, ws_s.at[0], ws_r.at[s, m], at_fs(source(hop))).start()
        remote(ref, ref, yw_s.at[0], yw_r.at[0], partner).start()

    def pass_routed(i, m):
        s = source(i)
        ref = wout_ref.at[0, m, s, g]
        with scope(f"E{i}{m}"):
            landed(ref, we_r.at[s, m])
        remote(ref, ref, yw_s.at[0], yw_r.at[0], partner).start()

    def start_up():
        for d in tp_others:
            remote(ssown, ssbuf.at[t], ss_s.at[0], ss_r.at[0], at_tp(d)).start()
        convert(0)
        convert(1)
        forward_block(0)
        squares = ssown[...]
        with scope("sswait"):
            landed(ssbuf.at[three], ss_r.at[0])
        for d in tp_others:
            squares = squares + ssbuf[d]
        scown[...] = lax.rsqrt(squares / (width * n_tp) + norm_eps)
        for d in fs_others:
            remote(scown, scbuf.at[f], sc_s.at[0], sc_r.at[f], at_fs(d)).start()
        convert(2)

    def keep_own():
        for h in range(2):
            wout_ref[0, :, f, h] = wall[:, f, h * half : (h + 1) * half]
            wout_ref[1, :, f, h] = wall[:, experts, h * half : (h + 1) * half]

    def finish():
        mixed_ref[...] = acc[0].astype(bf16)

    @pl.when(at_edge)
    def _():
        meta_to(1, f)
        for h in range(2):
            tokens_to(1, f, h)
        start_up()
        give_shared(1)
        for i in range(1, n_fs):
            give_expert(i)
        keep_own()
        take_tokens(1, 0)
        take_tokens(1, 1)
        forward_block(1)
        hidden_block(0)
        take_tokens(2, 0)
        take_tokens(2, 1)
        forward_block(2)
        hidden_block(1)
        down_block(0)
        pass_shared(1, 0)
        take_tokens(3, 0)
        take_tokens(3, 1)
        forward_block(3)
        hidden_block(2)
        down_block(1)
        chain_start(1)
        pass_shared(1, 1)
        pass_routed(3, 0)
        hidden_block(3)
        pass_routed(3, 1)
        pass_routed(3, 2)
        down_block(2)
        pass_shared(1, 2)
        down_block(3)
        chain_start(3)
        chain_start(2)
        for m in range(3):
            pass_routed(1, m)
        pass_shared(2, 0)
        pass_shared(2, 1)
        for m in range(3):
            pass_routed(2, m)
        pass_shared(2, 2)
        for m in range(3):
            pass_shared(3, m)
        for h in range(2):
            chain_end(f + (n_fs - f) * (1 - jnp.minimum(1, f)), h)
        finish()
        sent(tokbuf.at[0], tok_s.at[0])
        sent(metabuf.at[0], meta_s.at[0])
        sent(wall.at[:, 0, pl.ds(0, half)], ws_s.at[0])

    @pl.when(inside)
    def _():
        for hop in (1, 2):
            meta_to(hop, f)
        for h in range(2):
            for hop in (1, 2):
                tokens_to(hop, f, h)
        start_up()
        for h in range(2):
            take_tokens(2, h, hop=1)
            take_tokens(1, h, hop=2)
        give_shared(1, (0,))
        give_shared(2)
        give_expert(2)
        forward_block(1)
        forward_block(2)
        hidden_block(0)
        for h in range(2):
            take_tokens(3, h, hop=1)
        give_shared(1, (1, 2))
        give_expert(1)
        forward_block(3)
        keep_own()
        for m in range(3):
            pass_shared(1, m, hop=2)
        give_expert(3)
        hidden_block(1)
        hidden_block(2)
        for m in range(3):
            pass_routed(1, m)
        down_block(0)
        hidden_block(3)
        pass_shared(2, 0, hop=1)
        pass_shared(2, 1, hop=1)
        down_block(1)
        down_block(2)
        down_block(3)
        pass_shared(2, 2, hop=1)
        for m in range(3):
            pass_routed(2, m)
        for m in range(3):
            pass_shared(3, m, hop=1)
        for m in range(3):
            pass_routed(3, m)
        for i in (3, 2, 1):
            for h in range(2):
                chain_on(i, h)
        for h in range(2):
            chain_end(f, h)
            chain_end(n_fs, h)
        finish()
        sent(chain, tok_s.at[0])
        sent(metabuf, meta_s.at[0])
        sent(wall.at[:, :, pl.ds(0, half)], ws_s.at[0])

    with scope("ywait"):
        landed(wout_ref.at[:, :, pl.ds(0, n_fs - 1), 0], yw_r.at[0])

    with scope("drain"):
        sent(ssbuf.at[three], ss_s.at[0])
        sent(scbuf.at[pl.ds(0, n_fs - 1)], sc_s.at[0])
        sent(rsbuf.at[:, three], rs_s.at[0])
        sent(hid.at[:, three], ag_s.at[0])
        sent(outb.at[pl.ds(0, n_fs - 1)], ch_s.at[0])
        sent(wout_ref.at[0, :, pl.ds(0, n_fs - 1), 0], we_s.at[0])
        sent(wout_ref.at[:, :, pl.ds(0, n_fs - 1), 0], yw_s.at[0])


def put_out(mixed_ref, served_ref, *rest):
    outs, sems = rest[:-1], rest[-1]
    copies = [pltpu.make_async_copy(served_ref.at[i], outs[1 + i], sems.at[1 + i]) for i in range(len(outs) - 1)]
    copies.append(pltpu.make_async_copy(mixed_ref, outs[0], sems.at[0]))
    for copy in copies:
        copy.start()
    for copy in copies:
        copy.wait()


def per_device_fused(
    tokens,
    routes,
    routing_weight,
    norm_gain_vector,
    expert_gate,
    expert_up,
    expert_down,
    shared_gate,
    shared_up,
    shared_down,
):
    n_fs, n_tp = lax.axis_size("fs"), lax.axis_size("tp")
    rows, width = tokens.shape
    experts, units, _ = expert_gate.shape
    top_count = routes.shape[1]
    sub, half = rows // n_tp, units // 2
    meta_rows = -(-2 * top_count // 8) * 8
    lanes = -(-rows // 128) * 128
    f32, bf16 = jnp.float32, jnp.bfloat16
    kinds = top_count + 1
    dma = pltpu.SemaphoreType.DMA
    vmem = pl.BlockSpec(memory_space=pltpu.VMEM)
    hbm = pl.BlockSpec(memory_space=pltpu.HBM)
    mixed, served = pl.pallas_call(
        functools.partial(fused_kernel, n_fs, n_tp, top_count),
        out_shape=(
            pltpu.VMEM((rows, width), bf16),
            pltpu.VMEM((2, 3, n_fs, 2, half, width), bf16),
        ),
        in_specs=[hbm] * 10,
        out_specs=(vmem, vmem),
        scratch_shapes=[
            pltpu.VMEM((3, experts + 1, units, width), f32),
            pltpu.VMEM((top_count, rows), jnp.int32),
            pltpu.VMEM((top_count, rows), f32),
            pltpu.VMEM((1, width), f32),
            pltpu.VMEM((3, experts + 1, units, width), bf16),
            pltpu.VMEM((n_fs, rows, width), bf16),
            pltpu.VMEM((meta_rows, lanes), f32),
            pltpu.VMEM((n_fs + 1, meta_rows, lanes), f32),
            pltpu.VMEM((8, lanes), f32),
            pltpu.VMEM((n_tp, 8, lanes), f32),
            pltpu.VMEM((8, lanes), f32),
            pltpu.VMEM((n_fs, 8, lanes), f32),
            pltpu.VMEM((n_fs, rows, meta_rows), f32),
            pltpu.VMEM((n_fs, rows, 8), f32),
            pltpu.VMEM((n_fs, n_tp, sub, 2 * kinds * units), bf16),
            pltpu.VMEM((n_fs, n_tp, sub, 2 * kinds * units), bf16),
            pltpu.VMEM((n_fs, n_tp, sub, kinds * units), bf16),
            pltpu.VMEM((n_fs, rows, width), f32),
            pltpu.VMEM((n_fs, rows, width), bf16),
            pltpu.VMEM((n_fs + 1, rows, width), bf16),
            dma((7,)),
            dma((1,)), dma((n_fs, 2)),
            dma((1,)), dma((n_fs,)),
            dma((1,)), dma((1,)),
            dma((1,)), dma((n_fs,)),
            dma((1,)), dma((n_fs,)),
            dma((1,)), dma((n_fs,)),
            dma((1,)), dma((n_fs + 1, 2)),
            dma((1,)), dma((n_fs, 3)),
            dma((1,)), dma((n_fs, 3)),
            dma((1,)), dma((1,)),
        ],
        compiler_params=pltpu.CompilerParams(
            collective_id=0, has_side_effects=True, vmem_limit_bytes=40 * 1024 * 1024
        ),
        name="hand_over_and_layer",
    )(*[
        pltpu.with_memory_space_constraint(value, pltpu.HBM)
        for value in (
            tokens, routes.T, routing_weight.T, norm_gain_vector[None, :],
            expert_gate, expert_up, expert_down, shared_gate, shared_up, shared_down,
        )
    ])
    units_all = n_fs * units
    outs = pl.pallas_call(
        put_out,
        out_shape=(
            jax.ShapeDtypeStruct((rows, width), bf16),
            *[jax.ShapeDtypeStruct((units_all, width), bf16)] * 6,
        ),
        in_specs=[vmem] * 2,
        out_specs=(hbm,) * 7,
        scratch_shapes=[dma((7,))],
        compiler_params=pltpu.CompilerParams(vmem_limit_bytes=8 * 1024 * 1024),
        name="put_out",
    )(mixed, served.reshape(6, units_all, width))
    return (outs[0], outs[1][None], outs[2][None], outs[3][None], *outs[4:])


def per_device(tokens, routes, routing_weight, norm_gain_vector, *weights):
    experts, units, width = weights[0].shape
    rows, n_fs, n_tp = tokens.shape[0], lax.axis_size("fs"), lax.axis_size("tp")
    whole_tiles = units % 128 == 0 and width % 128 == 0 and rows % (16 * n_tp) == 0
    fits = (experts + 1) * units * width <= 2**20 and n_fs == 4 and n_tp <= 4
    chosen = per_device_plain
    if whole_tiles and fits and experts == n_fs and lax.axis_size("grp") == 2:
        chosen = per_device_fused
    return chosen(tokens, routes, routing_weight, norm_gain_vector, *weights)


def solution(mesh):
    return jax.shard_map(
        per_device,
        mesh=mesh,
        in_specs=(
            P(("grp", "fs"), "tp"),
            P(("grp", "fs"), None),
            P(("grp", "fs"), None),
            P("tp"),
            P(None, "fs", "tp"),
            P(None, "fs", "tp"),
            P(None, "fs", "tp"),
            P("fs", "tp"),
            P("fs", "tp"),
            P("fs", "tp"),
        ),
        out_specs=(
            P(("grp", "fs"), "tp"),
            P(("grp", "fs"), None, "tp"),
            P(("grp", "fs"), None, "tp"),
            P(("grp", "fs"), None, "tp"),
            P("grp", "tp"),
            P("grp", "tp"),
            P("grp", "tp"),
        ),
        check_vma=False,
    )
```

```python
import functools

import jax
import jax.numpy as jnp
from jax import lax
from jax.experimental import pallas as pl
from jax.experimental.pallas import tpu as pltpu
from jax.sharding import PartitionSpec as P

norm_eps = 1e-06


def dense_rows(rows, weight):
    return lax.dot_general(
        rows, weight, (((1,), (1,)), ((), ())), preferred_element_type=jnp.float32
    )


def per_device_plain(
    tokens,
    routes,
    routing_weight,
    norm_gain_vector,
    expert_gate,
    expert_up,
    expert_down,
    shared_gate,
    shared_up,
    shared_down,
):
    tok_rows, portion_width = tokens.shape
    model_width = portion_width * lax.axis_size("tp")
    experts = expert_gate.shape[0]
    top_count = routes.shape[1]
    capacity = tok_rows * top_count * 7 // (6 * experts)
    gate_round = (expert_gate * norm_gain_vector[None, None, :]).astype(jnp.bfloat16)
    up_round = (expert_up * norm_gain_vector[None, None, :]).astype(jnp.bfloat16)
    down_round = expert_down.astype(jnp.bfloat16)
    gate_refreshed, up_new, down_new = (
        lax.all_to_all(gate_round, "fs", split_axis=0, concat_axis=1, tiled=True),
        lax.all_to_all(up_round, "fs", split_axis=0, concat_axis=1, tiled=True),
        lax.all_to_all(down_round, "fs", split_axis=0, concat_axis=1, tiled=True),
    )
    shared_g, shared_u, shared_d = (
        lax.all_gather(
            (shared_gate * norm_gain_vector[None, :]).astype(jnp.bfloat16), "fs", axis=0, tiled=True
        ),
        lax.all_gather(
            (shared_up * norm_gain_vector[None, :]).astype(jnp.bfloat16), "fs", axis=0, tiled=True
        ),
        lax.all_gather(shared_down.astype(jnp.bfloat16), "fs", axis=0, tiled=True),
    )
    values = tokens.astype(jnp.float32)
    totals = lax.psum(jnp.sum(values * values, axis=1), "tp")
    normed = (values * lax.rsqrt(totals / model_width + norm_eps)[:, None]).astype(jnp.bfloat16)
    flat_expert = routes.reshape(-1)
    onehot = (flat_expert[:, None] == jnp.arange(experts, dtype=jnp.int32)[None, :]).astype(
        jnp.int32
    )
    earlier = jnp.cumsum(onehot, axis=0) - onehot
    slot_index = jnp.sum(earlier * onehot, axis=1)
    target = (flat_expert * capacity + slot_index).reshape(tok_rows, top_count)
    places = jnp.arange(experts * capacity, dtype=jnp.int32)
    placing = jnp.sum(
        (target[:, :, None] == places[None, None, :]).astype(jnp.int32), axis=1
    ).astype(jnp.bfloat16)
    outgoing = lax.dot_general(
        placing, normed, (((0,), (0,)), ((), ())), preferred_element_type=jnp.float32
    ).astype(jnp.bfloat16)
    incoming = lax.all_to_all(
        outgoing.reshape(experts, capacity, portion_width),
        "fs",
        split_axis=0,
        concat_axis=0,
        tiled=True,
    )
    arrived = incoming.reshape(experts * capacity, portion_width)
    partials = (
        dense_rows(arrived, gate_refreshed[0]).astype(jnp.bfloat16),
        dense_rows(arrived, up_new[0]).astype(jnp.bfloat16),
        dense_rows(normed, shared_g).astype(jnp.bfloat16),
        dense_rows(normed, shared_u).astype(jnp.bfloat16),
    )
    gate_part, up_part, sgate_part, sup_part = (
        lax.psum_scatter(partials[0], "tp", scatter_dimension=1, tiled=True).astype(jnp.float32),
        lax.psum_scatter(partials[1], "tp", scatter_dimension=1, tiled=True).astype(jnp.float32),
        lax.psum_scatter(partials[2], "tp", scatter_dimension=1, tiled=True).astype(jnp.float32),
        lax.psum_scatter(partials[3], "tp", scatter_dimension=1, tiled=True).astype(jnp.float32),
    )
    hidden, shared_hidden = (
        lax.all_gather(
            (jax.nn.silu(gate_part) * up_part).astype(jnp.bfloat16), "tp", axis=1, tiled=True
        ),
        lax.all_gather(
            (jax.nn.silu(sgate_part) * sup_part).astype(jnp.bfloat16), "tp", axis=1, tiled=True
        ),
    )
    produced = jnp.dot(hidden, down_new[0], preferred_element_type=jnp.float32).astype(jnp.bfloat16)
    returned = lax.all_to_all(
        produced.reshape(experts, capacity, portion_width),
        "fs",
        split_axis=0,
        concat_axis=0,
        tiled=True,
    )
    picked = returned.reshape(experts * capacity, portion_width)[target]
    routed = jnp.sum(routing_weight[:, :, None] * picked.astype(jnp.float32), axis=1)
    shared_out = jnp.dot(shared_hidden, shared_d, preferred_element_type=jnp.float32)
    mixed = (routed + shared_out).astype(jnp.bfloat16)
    return (mixed, gate_refreshed, up_new, down_new, shared_g, shared_u, shared_d)


MESH = pl.DeviceIdType.MESH


def outward_first(n):
    def key(f):
        return lambda s: (abs(s - f), abs(2 * s - n + 1) <= abs(2 * f - n + 1), s)

    orders = [sorted(range(n), key=key(f)) for f in range(n)]
    return [sum(orders[f][i] * n**f for f in range(n)) for i in range(n)]


def fused_kernel(
    n_fs, n_tp, top_count,
    tok_in, routes_in, weight_in, gain_in, eg_in, eu_in, ed_in, sg_in, su_in, sd_in,
    mixed_ref, wout_ref,
    raw, routes_ref, weight_ref, gain_ref,
    wall, tokbuf, meta_ref, metabuf, ssown, ssbuf, mt, part, rsbuf, hid, acc, outb, chain,
    in_s, tok_s, tok_r, meta_s, meta_r, ss_s, ss_r, rs_s, rs_r, ag_s, ag_r,
    ch_s, ch_r, we_s, we_r, ws_s, ws_r, yw_s, yw_r,
):
    g, f, t = lax.axis_index("grp"), lax.axis_index("fs"), lax.axis_index("tp")
    rows, width = tokbuf.shape[1:]
    experts, units = eg_in.shape[0], eg_in.shape[1]
    sub = rows // n_tp
    half = units // 2
    f32, bf16 = jnp.float32, jnp.bfloat16
    code = outward_first(n_fs)
    scope = jax.named_scope
    parts = [pl.ds(h * (rows // 2), rows // 2) for h in range(2)]
    three = pl.ds(0, n_tp - 1)

    def source(i):
        total = 0
        digits = code[i]
        picks = [(digits // n_fs**q) % n_fs for q in range(n_fs)]
        for q in range(n_fs):
            hit = 1 - jnp.minimum(1, jnp.abs(f - q))
            total = total + picks[q] * hit
        return total

    at_edge = (f == 0) | (f == n_fs - 1)
    inside = (f > 0) & (f < n_fs - 1)

    def at_fs(index):
        return (g, index, t)

    def at_tp(index):
        return (g, f, index)

    partner = (1 - g, f, t)

    def remote(src, dst, send, recv, device):
        return pltpu.make_async_remote_copy(
            src_ref=src, dst_ref=dst, send_sem=send, recv_sem=recv,
            device_id=device, device_id_type=MESH,
        )

    def sent(ref, send):
        remote(ref, ref, send, send, partner).wait_send()

    def landed(ref, recv):
        remote(ref, ref, recv, recv, partner).wait_recv()

    tp_others = [lax.rem(t + j, n_tp) for j in range(1, n_tp)]

    barrier = pltpu.get_barrier_semaphore()

    def greet(device):
        pl.semaphore_signal(barrier, inc=1, device_id=device, device_id_type=MESH)

    @pl.when(f > 0)
    def _():
        greet(at_fs(f - 1))

    @pl.when(f < n_fs - 1)
    def _():
        greet(at_fs(f + 1))

    for device in [at_tp(d) for d in tp_others] + [partner]:
        greet(device)

    small = [
        pltpu.make_async_copy(tok_in, tokbuf.at[f], in_s.at[0]),
        pltpu.make_async_copy(routes_in, routes_ref, in_s.at[1]),
        pltpu.make_async_copy(weight_in, weight_ref, in_s.at[2]),
        pltpu.make_async_copy(gain_in, gain_ref, in_s.at[3]),
    ]
    for load in small:
        load.start()
    for m, (routed, shared) in enumerate(((eg_in, sg_in), (eu_in, su_in), (ed_in, sd_in))):
        pltpu.make_async_copy(routed, raw.at[m, pl.ds(0, experts)], in_s.at[4 + m]).start()
        pltpu.make_async_copy(shared, raw.at[m, experts], in_s.at[4 + m]).start()
    small[0].wait()
    with scope("barrier"):
        pl.semaphore_wait(barrier, n_tp + jnp.minimum(1, f) + jnp.minimum(1, n_fs - 1 - f))

    def convert(m):
        pltpu.make_async_copy(raw.at[m], raw.at[m], in_s.at[4 + m]).wait()
        for e in range(experts + 1):
            value = raw[m, e]
            wall[m, e] = (value * gain_ref[...] if m < 2 else value).astype(bf16)

    def transposed(row_ref):
        return jnp.transpose(row_ref[...])[0:rows]

    def forward_block(i):
        s = source(i)
        with scope(f"fwd{i}"):
            mt[i] = transposed(meta_ref if i == 0 else metabuf.at[s])
            tokens = tokbuf[s]
            names = [mt[i, :, k : k + 1] for k in range(top_count)]
            columns = []
            for m in range(2):
                weight = wall[m].reshape((experts + 1) * units, width)
                sums = dense_rows(tokens, weight)
                for name in names:
                    chosen = jnp.zeros((rows, units), f32)
                    for e in range(experts):
                        chosen = jnp.where(name == float(e), sums[:, e * units : (e + 1) * units], chosen)
                    columns.append(chosen)
                columns.append(sums[:, experts * units :])
            for c, column in enumerate(columns):
                part[i, :, :, c * units : (c + 1) * units] = column.astype(bf16).reshape(n_tp, sub, units)
            for d in tp_others:
                remote(part.at[i, d], rsbuf.at[i, t], rs_s.at[0], rs_r.at[i], at_tp(d)).start()

    def hidden_block(i):
        with scope(f"hid{i}"):
            own_rows = pl.ds(pl.multiple_of(t * sub, 8), sub)
            weights = mt[i, own_rows, :]
            scale = weights[:, 2 * top_count : 2 * top_count + 1]
            landed(rsbuf.at[i, three], rs_r.at[i])
            total = part[i, t].astype(f32)
            for d in tp_others:
                total = total + rsbuf[i, d].astype(f32)
            total = total * scale
            kinds = top_count + 1
            for k in range(kinds):
                gate = total[:, k * units : (k + 1) * units]
                up = total[:, (kinds + k) * units : (kinds + k + 1) * units]
                value = jax.nn.silu(gate) * up
                if k < top_count:
                    value = value * weights[:, top_count + k : top_count + k + 1]
                hid[i, t, :, k * units : (k + 1) * units] = value.astype(bf16)
            for d in tp_others:
                remote(hid.at[i, t], hid.at[i, t], ag_s.at[0], ag_r.at[i], at_tp(d)).start()

    def down_block(i):
        with scope(f"down{i}"):
            landed(hid.at[i, three], ag_r.at[i])
            values = hid[i].astype(f32).reshape(rows, (top_count + 1) * units)
            names = [mt[i, :, k : k + 1] for k in range(top_count)]
            spread = []
            for e in range(experts):
                chosen = jnp.zeros((rows, units), f32)
                for k, name in enumerate(names):
                    chosen = jnp.where(name == float(e), values[:, k * units : (k + 1) * units], chosen)
                spread.append(chosen.astype(bf16))
            spread.append(values[:, top_count * units :].astype(bf16))
            weight = wall[2].reshape((experts + 1) * units, width)
            acc[i] = jnp.dot(jnp.concatenate(spread, axis=1), weight, preferred_element_type=f32)

    def chain_send(i, h, hop, last):
        d = source(i)
        slot = d
        if last:
            slot = d + (n_fs - d) * jnp.minimum(1, jnp.maximum(0, f - d))
        remote(
            outb.at[i, parts[h]], chain.at[slot, parts[h]], ch_s.at[0], ch_r.at[slot, h], at_fs(source(hop))
        ).start()

    def chain_start(i):
        for h in range(2):
            outb[i, parts[h]] = acc[i, parts[h]].astype(bf16)
            chain_send(i, h, 1, i == 1)

    def chain_on(i, h):
        d = source(i)
        with scope(f"chain{i}{h}"):
            landed(chain.at[d, parts[h]], ch_r.at[d, h])
        outb[i, parts[h]] = (acc[i, parts[h]] + chain[d, parts[h]].astype(f32)).astype(bf16)
        chain_send(i, h, min(i, 2), i < 3)

    def chain_end(slot, h):
        with scope(f"last{h}"):
            landed(chain.at[slot, parts[h]], ch_r.at[slot, h])
        acc[0, parts[h]] = acc[0, parts[h]] + chain[slot, parts[h]].astype(f32)

    def tokens_to(hop, s, h):
        ref = tokbuf.at[s, parts[h]]
        remote(ref, ref, tok_s.at[0], tok_r.at[s, h], at_fs(source(hop))).start()

    def meta_to(hop, s):
        remote(
            meta_ref if s is f else metabuf.at[s], metabuf.at[s], meta_s.at[0], meta_r.at[s], at_fs(source(hop))
        ).start()

    def take_tokens(i, h, hop=None):
        s = source(i)
        with scope(f"tok{i}{h}"):
            landed(tokbuf.at[s, parts[h]], tok_r.at[s, h])
            if hop:
                tokens_to(hop, s, h)

    def take_small(i, hop=None):
        s = source(i)
        with scope(f"small{i}"):
            landed(metabuf.at[s], meta_r.at[s])
            if hop:
                meta_to(hop, s)

    mine = pl.ds(pl.multiple_of(g * half, 16), half)

    def give_shared(hop, pieces=(0, 1, 2)):
        for m in pieces:
            remote(
                wall.at[m, experts, mine], wout_ref.at[1, m, f, g], ws_s.at[0], ws_r.at[f, m], at_fs(source(hop))
            ).start()

    def give_expert(i):
        d = source(i)
        for m in range(3):
            remote(wall.at[m, d, mine], wout_ref.at[0, m, f, g], we_s.at[0], we_r.at[f, m], at_fs(d)).start()

    def pass_shared(i, m, hop=None):
        s = source(i)
        ref = wout_ref.at[1, m, s, g]
        with scope(f"S{i}{m}"):
            landed(ref, ws_r.at[s, m])
        if hop:
            remote(ref, ref, ws_s.at[0], ws_r.at[s, m], at_fs(source(hop))).start()
        remote(ref, ref, yw_s.at[0], yw_r.at[0], partner).start()

    def pass_routed(i, m):
        s = source(i)
        ref = wout_ref.at[0, m, s, g]
        with scope(f"E{i}{m}"):
            landed(ref, we_r.at[s, m])
        remote(ref, ref, yw_s.at[0], yw_r.at[0], partner).start()

    def start_up(hops):
        for load in small[1:]:
            load.wait()
        meta_ref[...] = jnp.zeros(meta_ref.shape, f32)
        meta_ref[0:top_count, 0:rows] = routes_ref[...].astype(f32)
        meta_ref[top_count : 2 * top_count, 0:rows] = weight_ref[...]
        x = tokbuf[f].astype(f32)
        sq = x * x
        high = sq.astype(bf16)
        low = (sq - high.astype(f32)).astype(bf16)
        ones = jnp.ones((8, width), bf16)
        ssown[...] = jnp.zeros(ssown.shape, f32)
        ssown[:, 0:rows] = dense_rows(ones, high) + dense_rows(ones, low)
        for d in tp_others:
            remote(ssown, ssbuf.at[t], ss_s.at[0], ss_r.at[0], at_tp(d)).start()
        convert(0)
        convert(1)
        forward_block(0)
        squares = ssown[...]
        with scope("sswait"):
            landed(ssbuf.at[three], ss_r.at[0])
        for d in tp_others:
            squares = squares + ssbuf[d]
        scale = lax.rsqrt(squares / (width * n_tp) + norm_eps)
        meta_ref[2 * top_count : 2 * top_count + 1] = scale[0:1]
        for hop in hops:
            meta_to(hop, f)
        mt[0] = transposed(meta_ref)
        convert(2)

    def keep_own():
        for h in range(2):
            wout_ref[0, :, f, h] = wall[:, f, h * half : (h + 1) * half]
            wout_ref[1, :, f, h] = wall[:, experts, h * half : (h + 1) * half]

    def finish():
        mixed_ref[...] = acc[0].astype(bf16)

    @pl.when(at_edge)
    def _():
        for h in range(2):
            tokens_to(1, f, h)
        start_up((1,))
        give_shared(1)
        give_expert(1)
        keep_own()
        take_tokens(1, 0)
        take_tokens(1, 1)
        take_small(1)
        give_expert(2)
        forward_block(1)
        hidden_block(0)
        take_tokens(2, 0)
        take_tokens(2, 1)
        take_small(2)
        give_expert(3)
        forward_block(2)
        hidden_block(1)
        down_block(0)
        pass_shared(1, 0)
        take_tokens(3, 0)
        take_tokens(3, 1)
        take_small(3)
        forward_block(3)
        hidden_block(2)
        down_block(1)
        chain_start(1)
        pass_shared(1, 1)
        pass_shared(1, 2)
        pass_routed(3, 0)
        hidden_block(3)
        pass_routed(3, 1)
        pass_routed(3, 2)
        down_block(2)
        pass_routed(1, 0)
        down_block(3)
        chain_start(3)
        chain_start(2)
        pass_routed(1, 1)
        pass_routed(1, 2)
        pass_shared(2, 0)
        pass_shared(2, 1)
        pass_routed(2, 0)
        pass_shared(2, 2)
        pass_routed(2, 1)
        pass_routed(2, 2)
        for m in range(3):
            pass_shared(3, m)
        for h in range(2):
            chain_end(f + (n_fs - f) * (1 - jnp.minimum(1, f)), h)
        finish()
        sent(tokbuf.at[0], tok_s.at[0])
        sent(metabuf.at[0], meta_s.at[0])
        sent(wall.at[:, 0, pl.ds(0, half)], ws_s.at[0])

    @pl.when(inside)
    def _():
        for h in range(2):
            for hop in (1, 2):
                tokens_to(hop, f, h)
        start_up((1, 2))
        for h in range(2):
            take_tokens(2, h, hop=1)
            take_tokens(1, h, hop=2)
        take_small(2, hop=1)
        take_small(1, hop=2)
        give_shared(1, (0,))
        give_shared(2)
        give_expert(2)
        forward_block(1)
        forward_block(2)
        hidden_block(0)
        for h in range(2):
            take_tokens(3, h, hop=1)
        take_small(3, hop=1)
        give_shared(1, (1, 2))
        give_expert(1)
        forward_block(3)
        keep_own()
        for m in range(3):
            pass_shared(1, m, hop=2)
        give_expert(3)
        hidden_block(1)
        hidden_block(2)
        for m in range(3):
            pass_routed(1, m)
        down_block(0)
        hidden_block(3)
        pass_shared(2, 0, hop=1)
        pass_shared(2, 1, hop=1)
        down_block(1)
        down_block(2)
        down_block(3)
        pass_shared(2, 2, hop=1)
        for m in range(3):
            pass_routed(2, m)
        for m in range(3):
            pass_shared(3, m, hop=1)
        for m in range(3):
            pass_routed(3, m)
        for i, h in ((3, 0), (3, 1), (2, 0), (1, 0), (2, 1), (1, 1)):
            chain_on(i, h)
        for h in range(2):
            chain_end(f, h)
            chain_end(n_fs, h)
        finish()
        sent(chain, tok_s.at[0])
        sent(metabuf, meta_s.at[0])
        sent(wall.at[:, :, pl.ds(0, half)], ws_s.at[0])

    with scope("ywait"):
        landed(wout_ref.at[:, :, pl.ds(0, n_fs - 1), 0], yw_r.at[0])

    with scope("drain"):
        sent(ssbuf.at[three], ss_s.at[0])
        sent(rsbuf.at[:, three], rs_s.at[0])
        sent(hid.at[:, three], ag_s.at[0])
        sent(outb.at[pl.ds(0, n_fs - 1)], ch_s.at[0])
        sent(wout_ref.at[0, :, pl.ds(0, n_fs - 1), 0], we_s.at[0])
        sent(wout_ref.at[:, :, pl.ds(0, n_fs - 1), 0], yw_s.at[0])


def put_out(mixed_ref, served_ref, *rest):
    outs, sems = rest[:-1], rest[-1]
    copies = [pltpu.make_async_copy(served_ref.at[i], outs[1 + i], sems.at[1 + i]) for i in range(len(outs) - 1)]
    copies.append(pltpu.make_async_copy(mixed_ref, outs[0], sems.at[0]))
    for copy in copies:
        copy.start()
    for copy in copies:
        copy.wait()


def per_device_fused(
    tokens,
    routes,
    routing_weight,
    norm_gain_vector,
    expert_gate,
    expert_up,
    expert_down,
    shared_gate,
    shared_up,
    shared_down,
):
    n_fs, n_tp = lax.axis_size("fs"), lax.axis_size("tp")
    rows, width = tokens.shape
    experts, units, _ = expert_gate.shape
    top_count = routes.shape[1]
    sub, half = rows // n_tp, units // 2
    meta_rows = -(-(2 * top_count + 1) // 8) * 8
    lanes = -(-rows // 128) * 128
    f32, bf16 = jnp.float32, jnp.bfloat16
    kinds = top_count + 1
    dma = pltpu.SemaphoreType.DMA
    vmem = pl.BlockSpec(memory_space=pltpu.VMEM)
    hbm = pl.BlockSpec(memory_space=pltpu.HBM)
    mixed, served = pl.pallas_call(
        functools.partial(fused_kernel, n_fs, n_tp, top_count),
        out_shape=(
            pltpu.VMEM((rows, width), bf16),
            pltpu.VMEM((2, 3, n_fs, 2, half, width), bf16),
        ),
        in_specs=[hbm] * 10,
        out_specs=(vmem, vmem),
        scratch_shapes=[
            pltpu.VMEM((3, experts + 1, units, width), f32),
            pltpu.VMEM((top_count, rows), jnp.int32),
            pltpu.VMEM((top_count, rows), f32),
            pltpu.VMEM((1, width), f32),
            pltpu.VMEM((3, experts + 1, units, width), bf16),
            pltpu.VMEM((n_fs, rows, width), bf16),
            pltpu.VMEM((meta_rows, lanes), f32),
            pltpu.VMEM((n_fs + 1, meta_rows, lanes), f32),
            pltpu.VMEM((8, lanes), f32),
            pltpu.VMEM((n_tp, 8, lanes), f32),
            pltpu.VMEM((n_fs, rows, meta_rows), f32),
            pltpu.VMEM((n_fs, n_tp, sub, 2 * kinds * units), bf16),
            pltpu.VMEM((n_fs, n_tp, sub, 2 * kinds * units), bf16),
            pltpu.VMEM((n_fs, n_tp, sub, kinds * units), bf16),
            pltpu.VMEM((n_fs, rows, width), f32),
            pltpu.VMEM((n_fs, rows, width), bf16),
            pltpu.VMEM((n_fs + 1, rows, width), bf16),
            dma((7,)),
            dma((1,)), dma((n_fs, 2)),
            dma((1,)), dma((n_fs,)),
            dma((1,)), dma((1,)),
            dma((1,)), dma((n_fs,)),
            dma((1,)), dma((n_fs,)),
            dma((1,)), dma((n_fs + 1, 2)),
            dma((1,)), dma((n_fs, 3)),
            dma((1,)), dma((n_fs, 3)),
            dma((1,)), dma((1,)),
        ],
        compiler_params=pltpu.CompilerParams(
            collective_id=0, has_side_effects=True, vmem_limit_bytes=40 * 1024 * 1024
        ),
        name="hand_over_and_layer",
    )(*[
        pltpu.with_memory_space_constraint(value, pltpu.HBM)
        for value in (
            tokens, routes.T, routing_weight.T, norm_gain_vector[None, :],
            expert_gate, expert_up, expert_down, shared_gate, shared_up, shared_down,
        )
    ])
    units_all = n_fs * units
    outs = pl.pallas_call(
        put_out,
        out_shape=(
            jax.ShapeDtypeStruct((rows, width), bf16),
            *[jax.ShapeDtypeStruct((units_all, width), bf16)] * 6,
        ),
        in_specs=[vmem] * 2,
        out_specs=(hbm,) * 7,
        scratch_shapes=[dma((7,))],
        compiler_params=pltpu.CompilerParams(vmem_limit_bytes=8 * 1024 * 1024),
        name="put_out",
    )(mixed, served.reshape(6, units_all, width))
    return (outs[0], outs[1][None], outs[2][None], outs[3][None], *outs[4:])


def per_device(tokens, routes, routing_weight, norm_gain_vector, *weights):
    experts, units, width = weights[0].shape
    rows, n_fs, n_tp = tokens.shape[0], lax.axis_size("fs"), lax.axis_size("tp")
    whole_tiles = units % 128 == 0 and width % 128 == 0 and rows % (16 * n_tp) == 0
    fits = (experts + 1) * units * width <= 2**20 and n_fs == 4 and n_tp <= 4
    chosen = per_device_plain
    if whole_tiles and fits and experts == n_fs and lax.axis_size("grp") == 2:
        chosen = per_device_fused
    return chosen(tokens, routes, routing_weight, norm_gain_vector, *weights)


def solution(mesh):
    return jax.shard_map(
        per_device,
        mesh=mesh,
        in_specs=(
            P(("grp", "fs"), "tp"),
            P(("grp", "fs"), None),
            P(("grp", "fs"), None),
            P("tp"),
            P(None, "fs", "tp"),
            P(None, "fs", "tp"),
            P(None, "fs", "tp"),
            P("fs", "tp"),
            P("fs", "tp"),
            P("fs", "tp"),
        ),
        out_specs=(
            P(("grp", "fs"), "tp"),
            P(("grp", "fs"), None, "tp"),
            P(("grp", "fs"), None, "tp"),
            P(("grp", "fs"), None, "tp"),
            P("grp", "tp"),
            P("grp", "tp"),
            P("grp", "tp"),
        ),
        check_vma=False,
    )
```

```python
import functools

import jax
import jax.numpy as jnp
from jax import lax
from jax.experimental import pallas as pl
from jax.experimental.pallas import tpu as pltpu
from jax.sharding import PartitionSpec as P

norm_eps = 1e-06


def dense_rows(rows, weight):
    return lax.dot_general(
        rows, weight, (((1,), (1,)), ((), ())), preferred_element_type=jnp.float32
    )


def per_device_plain(
    tokens,
    routes,
    routing_weight,
    norm_gain_vector,
    expert_gate,
    expert_up,
    expert_down,
    shared_gate,
    shared_up,
    shared_down,
):
    tok_rows, portion_width = tokens.shape
    model_width = portion_width * lax.axis_size("tp")
    experts = expert_gate.shape[0]
    top_count = routes.shape[1]
    capacity = tok_rows * top_count * 7 // (6 * experts)
    gate_round = (expert_gate * norm_gain_vector[None, None, :]).astype(jnp.bfloat16)
    up_round = (expert_up * norm_gain_vector[None, None, :]).astype(jnp.bfloat16)
    down_round = expert_down.astype(jnp.bfloat16)
    gate_refreshed, up_new, down_new = (
        lax.all_to_all(gate_round, "fs", split_axis=0, concat_axis=1, tiled=True),
        lax.all_to_all(up_round, "fs", split_axis=0, concat_axis=1, tiled=True),
        lax.all_to_all(down_round, "fs", split_axis=0, concat_axis=1, tiled=True),
    )
    shared_g, shared_u, shared_d = (
        lax.all_gather(
            (shared_gate * norm_gain_vector[None, :]).astype(jnp.bfloat16), "fs", axis=0, tiled=True
        ),
        lax.all_gather(
            (shared_up * norm_gain_vector[None, :]).astype(jnp.bfloat16), "fs", axis=0, tiled=True
        ),
        lax.all_gather(shared_down.astype(jnp.bfloat16), "fs", axis=0, tiled=True),
    )
    values = tokens.astype(jnp.float32)
    totals = lax.psum(jnp.sum(values * values, axis=1), "tp")
    normed = (values * lax.rsqrt(totals / model_width + norm_eps)[:, None]).astype(jnp.bfloat16)
    flat_expert = routes.reshape(-1)
    onehot = (flat_expert[:, None] == jnp.arange(experts, dtype=jnp.int32)[None, :]).astype(
        jnp.int32
    )
    earlier = jnp.cumsum(onehot, axis=0) - onehot
    slot_index = jnp.sum(earlier * onehot, axis=1)
    target = (flat_expert * capacity + slot_index).reshape(tok_rows, top_count)
    places = jnp.arange(experts * capacity, dtype=jnp.int32)
    placing = jnp.sum(
        (target[:, :, None] == places[None, None, :]).astype(jnp.int32), axis=1
    ).astype(jnp.bfloat16)
    outgoing = lax.dot_general(
        placing, normed, (((0,), (0,)), ((), ())), preferred_element_type=jnp.float32
    ).astype(jnp.bfloat16)
    incoming = lax.all_to_all(
        outgoing.reshape(experts, capacity, portion_width),
        "fs",
        split_axis=0,
        concat_axis=0,
        tiled=True,
    )
    arrived = incoming.reshape(experts * capacity, portion_width)
    partials = (
        dense_rows(arrived, gate_refreshed[0]).astype(jnp.bfloat16),
        dense_rows(arrived, up_new[0]).astype(jnp.bfloat16),
        dense_rows(normed, shared_g).astype(jnp.bfloat16),
        dense_rows(normed, shared_u).astype(jnp.bfloat16),
    )
    gate_part, up_part, sgate_part, sup_part = (
        lax.psum_scatter(partials[0], "tp", scatter_dimension=1, tiled=True).astype(jnp.float32),
        lax.psum_scatter(partials[1], "tp", scatter_dimension=1, tiled=True).astype(jnp.float32),
        lax.psum_scatter(partials[2], "tp", scatter_dimension=1, tiled=True).astype(jnp.float32),
        lax.psum_scatter(partials[3], "tp", scatter_dimension=1, tiled=True).astype(jnp.float32),
    )
    hidden, shared_hidden = (
        lax.all_gather(
            (jax.nn.silu(gate_part) * up_part).astype(jnp.bfloat16), "tp", axis=1, tiled=True
        ),
        lax.all_gather(
            (jax.nn.silu(sgate_part) * sup_part).astype(jnp.bfloat16), "tp", axis=1, tiled=True
        ),
    )
    produced = jnp.dot(hidden, down_new[0], preferred_element_type=jnp.float32).astype(jnp.bfloat16)
    returned = lax.all_to_all(
        produced.reshape(experts, capacity, portion_width),
        "fs",
        split_axis=0,
        concat_axis=0,
        tiled=True,
    )
    picked = returned.reshape(experts * capacity, portion_width)[target]
    routed = jnp.sum(routing_weight[:, :, None] * picked.astype(jnp.float32), axis=1)
    shared_out = jnp.dot(shared_hidden, shared_d, preferred_element_type=jnp.float32)
    mixed = (routed + shared_out).astype(jnp.bfloat16)
    return (mixed, gate_refreshed, up_new, down_new, shared_g, shared_u, shared_d)


MESH = pl.DeviceIdType.MESH


def outward_first(n):
    def key(f):
        return lambda s: (abs(s - f), abs(2 * s - n + 1) <= abs(2 * f - n + 1), s)

    orders = [sorted(range(n), key=key(f)) for f in range(n)]
    return [sum(orders[f][i] * n**f for f in range(n)) for i in range(n)]


def fused_kernel(
    n_fs, n_tp, top_count,
    tok_in, routes_in, weight_in, gain_in, eg_in, eu_in, ed_in, sg_in, su_in, sd_in,
    mixed_ref, wout_ref,
    raw, routes_ref, weight_ref, gain_ref,
    wall, tokbuf, meta_ref, metabuf, ssown, ssbuf, mt, part, rsbuf, hid, part_a, rsbuf_a, hid_a, part_b, rsbuf_b, hid_b, acc, outb, chain,
    in_s, tok_s, tok_r, meta_s, meta_r, ss_s, ss_r, rs_s, rs_r, ag_s, ag_r,
    ch_s, ch_r, we_s, we_r, ws_s, ws_r, yw_s, yw_r,
):
    g, f, t = lax.axis_index("grp"), lax.axis_index("fs"), lax.axis_index("tp")
    rows, width = tokbuf.shape[1:]
    experts, units = eg_in.shape[0], eg_in.shape[1]
    pieces = 3
    row_step = rows // pieces
    half = units // 2
    f32, bf16 = jnp.float32, jnp.bfloat16
    code = outward_first(n_fs)
    scope = jax.named_scope
    parts = [pl.ds(h * row_step, row_step) for h in range(pieces)]
    three = pl.ds(0, n_tp - 1)

    def source(i):
        total = 0
        digits = code[i]
        picks = [(digits // n_fs**q) % n_fs for q in range(n_fs)]
        for q in range(n_fs):
            hit = 1 - jnp.minimum(1, jnp.abs(f - q))
            total = total + picks[q] * hit
        return total

    at_edge = (f == 0) | (f == n_fs - 1)
    inside = (f > 0) & (f < n_fs - 1)

    def at_fs(index):
        return (g, index, t)

    def at_tp(index):
        return (g, f, index)

    partner = (1 - g, f, t)

    def remote(src, dst, send, recv, device):
        return pltpu.make_async_remote_copy(
            src_ref=src, dst_ref=dst, send_sem=send, recv_sem=recv,
            device_id=device, device_id_type=MESH,
        )

    def sent(ref, send):
        remote(ref, ref, send, send, partner).wait_send()

    def landed(ref, recv):
        remote(ref, ref, recv, recv, partner).wait_recv()

    tp_others = [lax.rem(t + j, n_tp) for j in range(1, n_tp)]

    barrier = pltpu.get_barrier_semaphore()

    def greet(device):
        pl.semaphore_signal(barrier, inc=1, device_id=device, device_id_type=MESH)

    @pl.when(f > 0)
    def _():
        greet(at_fs(f - 1))

    @pl.when(f < n_fs - 1)
    def _():
        greet(at_fs(f + 1))

    for device in [at_tp(d) for d in tp_others] + [partner]:
        greet(device)

    small = [
        pltpu.make_async_copy(tok_in, tokbuf.at[f], in_s.at[0]),
        pltpu.make_async_copy(routes_in, routes_ref, in_s.at[1]),
        pltpu.make_async_copy(weight_in, weight_ref, in_s.at[2]),
        pltpu.make_async_copy(gain_in, gain_ref, in_s.at[3]),
    ]
    for load in small:
        load.start()
    for m, (routed, shared) in enumerate(((eg_in, sg_in), (eu_in, su_in), (ed_in, sd_in))):
        pltpu.make_async_copy(routed, raw.at[m, pl.ds(0, experts)], in_s.at[4 + m]).start()
        pltpu.make_async_copy(shared, raw.at[m, experts], in_s.at[4 + m]).start()
    small[0].wait()
    with scope("barrier"):
        pl.semaphore_wait(barrier, n_tp + jnp.minimum(1, f) + jnp.minimum(1, n_fs - 1 - f))

    def convert(m):
        pltpu.make_async_copy(raw.at[m], raw.at[m], in_s.at[4 + m]).wait()
        for e in range(experts + 1):
            value = raw[m, e]
            wall[m, e] = (value * gain_ref[...] if m < 2 else value).astype(bf16)

    def transposed(row_ref):
        return jnp.transpose(row_ref[...])[0:rows]

    segments = [
        (i, 0, rows, part.at[i], rsbuf.at[i], hid.at[i]) for i in range(n_fs - 1)
    ] + [
        (n_fs - 1, 0, 2 * row_step, part_a, rsbuf_a, hid_a),
        (n_fs - 1, 2 * row_step, row_step, part_b, rsbuf_b, hid_b),
    ]

    def forward_block(q):
        i, first, count, part, rsbuf, _ = segments[q]
        span = pl.ds(first, count)
        s = source(i)
        with scope(f"fwd{q}"):
            if first == 0:
                mt[i] = transposed(meta_ref if i == 0 else metabuf.at[s])
            tokens = tokbuf[s, span]
            names = [mt[i, span, k : k + 1] for k in range(top_count)]
            columns = []
            for m in range(2):
                weight = wall[m].reshape((experts + 1) * units, width)
                sums = dense_rows(tokens, weight)
                for name in names:
                    chosen = jnp.zeros((count, units), f32)
                    for e in range(experts):
                        chosen = jnp.where(name == float(e), sums[:, e * units : (e + 1) * units], chosen)
                    columns.append(chosen)
                columns.append(sums[:, experts * units :])
            for c, column in enumerate(columns):
                part[:, :, c * units : (c + 1) * units] = column.astype(bf16).reshape(n_tp, count // n_tp, units)
            for d in tp_others:
                remote(part.at[d], rsbuf.at[t], rs_s.at[0], rs_r.at[q], at_tp(d)).start()

    def hidden_block(q):
        i, first, count, part, rsbuf, hid = segments[q]
        sub = count // n_tp
        with scope(f"hid{q}"):
            weights = mt[i, pl.ds(pl.multiple_of(first + t * sub, 8), sub), :]
            scale = weights[:, 2 * top_count : 2 * top_count + 1]
            landed(rsbuf.at[three], rs_r.at[q])
            total = part[t].astype(f32)
            for d in tp_others:
                total = total + rsbuf[d].astype(f32)
            total = total * scale
            kinds = top_count + 1
            for k in range(kinds):
                gate = total[:, k * units : (k + 1) * units]
                up = total[:, (kinds + k) * units : (kinds + k + 1) * units]
                value = jax.nn.silu(gate) * up
                if k < top_count:
                    value = value * weights[:, top_count + k : top_count + k + 1]
                hid[t, :, k * units : (k + 1) * units] = value.astype(bf16)
            for d in tp_others:
                remote(hid.at[t], hid.at[t], ag_s.at[0], ag_r.at[q], at_tp(d)).start()

    def down_block(q):
        i, first, count, _, _, hid = segments[q]
        span = pl.ds(first, count)
        with scope(f"down{q}"):
            landed(hid.at[three], ag_r.at[q])
            values = hid[...].astype(f32).reshape(count, (top_count + 1) * units)
            names = [mt[i, span, k : k + 1] for k in range(top_count)]
            spread = []
            for e in range(experts):
                chosen = jnp.zeros((count, units), f32)
                for k, name in enumerate(names):
                    chosen = jnp.where(name == float(e), values[:, k * units : (k + 1) * units], chosen)
                spread.append(chosen.astype(bf16))
            spread.append(values[:, top_count * units :].astype(bf16))
            weight = wall[2].reshape((experts + 1) * units, width)
            acc[i, span] = jnp.dot(jnp.concatenate(spread, axis=1), weight, preferred_element_type=f32)

    def chain_send(i, h, hop, last):
        d = source(i)
        slot = d
        if last:
            slot = d + (n_fs - d) * jnp.minimum(1, jnp.maximum(0, f - d))
        remote(
            outb.at[i, parts[h]], chain.at[slot, parts[h]], ch_s.at[0], ch_r.at[slot, h], at_fs(source(hop))
        ).start()

    def chain_start(i, which=(0, 1, 2)):
        for h in which:
            outb[i, parts[h]] = acc[i, parts[h]].astype(bf16)
            chain_send(i, h, 1, i == 1)

    def chain_on(i, h):
        d = source(i)
        with scope(f"chain{i}{h}"):
            landed(chain.at[d, parts[h]], ch_r.at[d, h])
        outb[i, parts[h]] = (acc[i, parts[h]] + chain[d, parts[h]].astype(f32)).astype(bf16)
        chain_send(i, h, min(i, 2), i < 3)

    def chain_end(slot, h):
        with scope(f"last{h}"):
            landed(chain.at[slot, parts[h]], ch_r.at[slot, h])
        acc[0, parts[h]] = acc[0, parts[h]] + chain[slot, parts[h]].astype(f32)

    def tokens_to(hop, s, h):
        ref = tokbuf.at[s, parts[h]]
        remote(ref, ref, tok_s.at[0], tok_r.at[s, h], at_fs(source(hop))).start()

    def meta_to(hop, s):
        remote(
            meta_ref if s is f else metabuf.at[s], metabuf.at[s], meta_s.at[0], meta_r.at[s], at_fs(source(hop))
        ).start()

    def take_tokens(i, h, hop=None):
        s = source(i)
        with scope(f"tok{i}{h}"):
            landed(tokbuf.at[s, parts[h]], tok_r.at[s, h])
            if hop:
                tokens_to(hop, s, h)

    def take_small(i, hop=None):
        s = source(i)
        with scope(f"small{i}"):
            landed(metabuf.at[s], meta_r.at[s])
            if hop:
                meta_to(hop, s)

    mine = pl.ds(pl.multiple_of(g * half, 16), half)

    def give_shared(hop, pieces=(0, 1, 2)):
        for m in pieces:
            remote(
                wall.at[m, experts, mine], wout_ref.at[1, m, f, g], ws_s.at[0], ws_r.at[f, m], at_fs(source(hop))
            ).start()

    def give_expert(i, pieces=(0, 1, 2)):
        d = source(i)
        for m in pieces:
            remote(wall.at[m, d, mine], wout_ref.at[0, m, f, g], we_s.at[0], we_r.at[f, m], at_fs(d)).start()

    def pass_shared(i, m, hop=None):
        s = source(i)
        ref = wout_ref.at[1, m, s, g]
        with scope(f"S{i}{m}"):
            landed(ref, ws_r.at[s, m])
        if hop:
            remote(ref, ref, ws_s.at[0], ws_r.at[s, m], at_fs(source(hop))).start()
        remote(ref, ref, yw_s.at[0], yw_r.at[0], partner).start()

    def pass_routed(i, m):
        s = source(i)
        ref = wout_ref.at[0, m, s, g]
        with scope(f"E{i}{m}"):
            landed(ref, we_r.at[s, m])
        remote(ref, ref, yw_s.at[0], yw_r.at[0], partner).start()

    def start_up(hops):
        for load in small[1:]:
            load.wait()
        meta_ref[...] = jnp.zeros(meta_ref.shape, f32)
        meta_ref[0:top_count, 0:rows] = routes_ref[...].astype(f32)
        meta_ref[top_count : 2 * top_count, 0:rows] = weight_ref[...]
        x = tokbuf[f].astype(f32)
        sq = x * x
        high = sq.astype(bf16)
        low = (sq - high.astype(f32)).astype(bf16)
        ones = jnp.ones((8, width), bf16)
        ssown[...] = jnp.zeros(ssown.shape, f32)
        ssown[:, 0:rows] = dense_rows(ones, high) + dense_rows(ones, low)
        for d in tp_others:
            remote(ssown, ssbuf.at[t], ss_s.at[0], ss_r.at[0], at_tp(d)).start()
        convert(0)
        if len(hops) > 1:
            give_shared(1, (0,))
            give_shared(2, (0,))
        convert(1)
        if len(hops) > 1:
            give_shared(1, (1,))
            tokens_to(1, f, 0)
        forward_block(0)
        squares = ssown[...]
        with scope("sswait"):
            landed(ssbuf.at[three], ss_r.at[0])
        for d in tp_others:
            squares = squares + ssbuf[d]
        scale = lax.rsqrt(squares / (width * n_tp) + norm_eps)
        meta_ref[2 * top_count : 2 * top_count + 1] = scale[0:1]
        for hop in hops:
            meta_to(hop, f)
        mt[0] = transposed(meta_ref)
        convert(2)

    def keep_own():
        for h in range(2):
            wout_ref[0, :, f, h] = wall[:, f, h * half : (h + 1) * half]
            wout_ref[1, :, f, h] = wall[:, experts, h * half : (h + 1) * half]

    def finish():
        mixed_ref[...] = acc[0].astype(bf16)

    @pl.when(at_edge)
    def _():
        for h in range(pieces):
            tokens_to(1, f, h)
        start_up((1,))
        give_shared(1)
        give_expert(1)
        keep_own()
        pass_shared(1, 0)
        pass_shared(1, 1)
        take_tokens(2, 0)
        give_expert(2)
        hidden_block(0)
        take_tokens(2, 1)
        take_tokens(2, 2)
        take_small(2)
        forward_block(2)
        down_block(0)
        pass_shared(1, 2)
        pass_routed(1, 0)
        take_tokens(3, 0)

        @pl.when(f > 0)
        def _():
            give_expert(3)

        pass_routed(1, 1)
        take_tokens(3, 1)
        take_tokens(3, 2)
        take_small(3)

        @pl.when(f == 0)
        def _():
            give_expert(3)

        forward_block(3)
        forward_block(4)
        hidden_block(2)
        pass_routed(3, 0)
        pass_routed(3, 1)
        hidden_block(3)
        hidden_block(4)
        pass_routed(3, 2)
        take_small(1)
        for h in range(pieces):
            take_tokens(1, h)
        forward_block(1)
        pass_routed(1, 2)
        down_block(3)
        chain_start(3, (0, 1))
        pass_shared(2, 0)
        down_block(4)
        chain_start(3, (2,))
        down_block(2)
        chain_start(2)
        pass_shared(2, 1)
        hidden_block(1)
        pass_routed(2, 0)
        pass_routed(2, 1)
        pass_shared(2, 2)
        pass_routed(2, 2)
        down_block(1)
        chain_start(1)
        for m in range(3):
            pass_shared(3, m)
        for h in range(pieces):
            chain_end(f + (n_fs - f) * (1 - jnp.minimum(1, f)), h)
        finish()
        sent(tokbuf.at[0], tok_s.at[0])
        sent(metabuf.at[0], meta_s.at[0])
        sent(wall.at[:, 0, pl.ds(0, half)], ws_s.at[0])

    @pl.when(inside)
    def _():
        for h in range(pieces):
            tokens_to(2, f, h)
        start_up((1, 2))
        for h in range(pieces):
            take_tokens(2, h, hop=1)
            take_tokens(1, h, hop=2)
        take_small(2, hop=1)
        take_small(1, hop=2)
        give_shared(1, (2,))
        give_expert(1, (0, 1))
        give_shared(2, (1, 2))
        give_expert(2)
        forward_block(1)
        forward_block(2)
        hidden_block(0)
        take_tokens(3, 0, hop=1)
        take_tokens(3, 1, hop=1)
        take_tokens(3, 2, hop=1)
        take_small(3, hop=1)
        for h in range(1, pieces):
            tokens_to(1, f, h)
        give_expert(1, (2,))
        forward_block(3)
        forward_block(4)
        keep_own()
        for m in range(3):
            pass_shared(1, m, hop=2)
        give_expert(3)
        hidden_block(1)
        hidden_block(2)
        for m in range(3):
            pass_routed(1, m)
        down_block(0)
        hidden_block(3)
        hidden_block(4)
        pass_shared(2, 0, hop=1)
        pass_shared(2, 1, hop=1)
        down_block(1)
        down_block(2)
        down_block(3)
        down_block(4)
        pass_shared(2, 2, hop=1)
        for m in range(3):
            pass_routed(2, m)
        for m in range(3):
            pass_shared(3, m, hop=1)
        for m in range(3):
            pass_routed(3, m)
        for i, h in ((3, 0), (3, 1), (3, 2), (2, 0), (1, 0), (2, 1), (1, 1), (2, 2), (1, 2)):
            chain_on(i, h)
        for h in range(pieces):
            chain_end(f, h)
            chain_end(n_fs, h)
        finish()
        sent(chain, tok_s.at[0])
        sent(metabuf, meta_s.at[0])
        sent(wall.at[:, :, pl.ds(0, half)], ws_s.at[0])

    with scope("ywait"):
        landed(wout_ref.at[:, :, pl.ds(0, n_fs - 1), 0], yw_r.at[0])

    with scope("drain"):
        sent(ssbuf.at[three], ss_s.at[0])
        sent(part, rs_s.at[0])
        sent(hid, ag_s.at[0])
        sent(outb.at[pl.ds(0, n_fs - 1)], ch_s.at[0])
        sent(wout_ref.at[0, :, pl.ds(0, n_fs - 1), 0], we_s.at[0])
        sent(wout_ref.at[:, :, pl.ds(0, n_fs - 1), 0], yw_s.at[0])


def put_out(mixed_ref, served_ref, *rest):
    outs, sems = rest[:-1], rest[-1]
    copies = [pltpu.make_async_copy(served_ref.at[i], outs[1 + i], sems.at[1 + i]) for i in range(len(outs) - 1)]
    copies.append(pltpu.make_async_copy(mixed_ref, outs[0], sems.at[0]))
    for copy in copies:
        copy.start()
    for copy in copies:
        copy.wait()


def per_device_fused(
    tokens,
    routes,
    routing_weight,
    norm_gain_vector,
    expert_gate,
    expert_up,
    expert_down,
    shared_gate,
    shared_up,
    shared_down,
):
    n_fs, n_tp = lax.axis_size("fs"), lax.axis_size("tp")
    rows, width = tokens.shape
    experts, units, _ = expert_gate.shape
    top_count = routes.shape[1]
    half = units // 2
    meta_rows = -(-(2 * top_count + 1) // 8) * 8
    lanes = -(-rows // 128) * 128
    f32, bf16 = jnp.float32, jnp.bfloat16
    kinds = top_count + 1
    dma = pltpu.SemaphoreType.DMA
    vmem = pl.BlockSpec(memory_space=pltpu.VMEM)
    hbm = pl.BlockSpec(memory_space=pltpu.HBM)
    mixed, served = pl.pallas_call(
        functools.partial(fused_kernel, n_fs, n_tp, top_count),
        out_shape=(
            pltpu.VMEM((rows, width), bf16),
            pltpu.VMEM((2, 3, n_fs, 2, half, width), bf16),
        ),
        in_specs=[hbm] * 10,
        out_specs=(vmem, vmem),
        scratch_shapes=[
            pltpu.VMEM((3, experts + 1, units, width), f32),
            pltpu.VMEM((top_count, rows), jnp.int32),
            pltpu.VMEM((top_count, rows), f32),
            pltpu.VMEM((1, width), f32),
            pltpu.VMEM((3, experts + 1, units, width), bf16),
            pltpu.VMEM((n_fs, rows, width), bf16),
            pltpu.VMEM((meta_rows, lanes), f32),
            pltpu.VMEM((n_fs + 1, meta_rows, lanes), f32),
            pltpu.VMEM((8, lanes), f32),
            pltpu.VMEM((n_tp, 8, lanes), f32),
            pltpu.VMEM((n_fs, rows, meta_rows), f32),
            *[
                pltpu.VMEM(lead + (n_tp, count // n_tp, times * kinds * units), bf16)
                for lead, count in (((n_fs - 1,), rows), ((), 2 * rows // 3), ((), rows // 3))
                for times in (2, 2, 1)
            ],
            pltpu.VMEM((n_fs, rows, width), f32),
            pltpu.VMEM((n_fs, rows, width), bf16),
            pltpu.VMEM((n_fs + 1, rows, width), bf16),
            dma((7,)),
            dma((1,)), dma((n_fs, 3)),
            dma((1,)), dma((n_fs,)),
            dma((1,)), dma((1,)),
            dma((1,)), dma((n_fs + 1,)),
            dma((1,)), dma((n_fs + 1,)),
            dma((1,)), dma((n_fs + 1, 3)),
            dma((1,)), dma((n_fs, 3)),
            dma((1,)), dma((n_fs, 3)),
            dma((1,)), dma((1,)),
        ],
        compiler_params=pltpu.CompilerParams(
            collective_id=0, has_side_effects=True, vmem_limit_bytes=40 * 1024 * 1024
        ),
        name="hand_over_and_layer",
    )(*[
        pltpu.with_memory_space_constraint(value, pltpu.HBM)
        for value in (
            tokens, routes.T, routing_weight.T, norm_gain_vector[None, :],
            expert_gate, expert_up, expert_down, shared_gate, shared_up, shared_down,
        )
    ])
    units_all = n_fs * units
    outs = pl.pallas_call(
        put_out,
        out_shape=(
            jax.ShapeDtypeStruct((rows, width), bf16),
            *[jax.ShapeDtypeStruct((units_all, width), bf16)] * 6,
        ),
        in_specs=[vmem] * 2,
        out_specs=(hbm,) * 7,
        scratch_shapes=[dma((7,))],
        compiler_params=pltpu.CompilerParams(vmem_limit_bytes=8 * 1024 * 1024),
        name="put_out",
    )(mixed, served.reshape(6, units_all, width))
    return (outs[0], outs[1][None], outs[2][None], outs[3][None], *outs[4:])


def per_device(tokens, routes, routing_weight, norm_gain_vector, *weights):
    experts, units, width = weights[0].shape
    rows, n_fs, n_tp = tokens.shape[0], lax.axis_size("fs"), lax.axis_size("tp")
    whole_tiles = units % 128 == 0 and width % 128 == 0 and rows % (48 * n_tp) == 0
    fits = (experts + 1) * units * width <= 2**20 and n_fs == 4 and n_tp <= 4
    chosen = per_device_plain
    if whole_tiles and fits and experts == n_fs and lax.axis_size("grp") == 2:
        chosen = per_device_fused
    return chosen(tokens, routes, routing_weight, norm_gain_vector, *weights)


def solution(mesh):
    return jax.shard_map(
        per_device,
        mesh=mesh,
        in_specs=(
            P(("grp", "fs"), "tp"),
            P(("grp", "fs"), None),
            P(("grp", "fs"), None),
            P("tp"),
            P(None, "fs", "tp"),
            P(None, "fs", "tp"),
            P(None, "fs", "tp"),
            P("fs", "tp"),
            P("fs", "tp"),
            P("fs", "tp"),
        ),
        out_specs=(
            P(("grp", "fs"), "tp"),
            P(("grp", "fs"), None, "tp"),
            P(("grp", "fs"), None, "tp"),
            P(("grp", "fs"), None, "tp"),
            P("grp", "tp"),
            P("grp", "tp"),
            P("grp", "tp"),
        ),
        check_vma=False,
    )
```

```python
import functools

import jax
import jax.numpy as jnp
from jax import lax
from jax.experimental import pallas as pl
from jax.experimental.pallas import tpu as pltpu
from jax.sharding import PartitionSpec as P

norm_eps = 1e-06


def dense_rows(rows, weight):
    return lax.dot_general(
        rows, weight, (((1,), (1,)), ((), ())), preferred_element_type=jnp.float32
    )


def per_device_plain(
    tokens,
    routes,
    routing_weight,
    norm_gain_vector,
    expert_gate,
    expert_up,
    expert_down,
    shared_gate,
    shared_up,
    shared_down,
):
    tok_rows, portion_width = tokens.shape
    model_width = portion_width * lax.axis_size("tp")
    experts = expert_gate.shape[0]
    top_count = routes.shape[1]
    capacity = tok_rows * top_count * 7 // (6 * experts)
    gate_round = (expert_gate * norm_gain_vector[None, None, :]).astype(jnp.bfloat16)
    up_round = (expert_up * norm_gain_vector[None, None, :]).astype(jnp.bfloat16)
    down_round = expert_down.astype(jnp.bfloat16)
    gate_refreshed, up_new, down_new = (
        lax.all_to_all(gate_round, "fs", split_axis=0, concat_axis=1, tiled=True),
        lax.all_to_all(up_round, "fs", split_axis=0, concat_axis=1, tiled=True),
        lax.all_to_all(down_round, "fs", split_axis=0, concat_axis=1, tiled=True),
    )
    shared_g, shared_u, shared_d = (
        lax.all_gather(
            (shared_gate * norm_gain_vector[None, :]).astype(jnp.bfloat16), "fs", axis=0, tiled=True
        ),
        lax.all_gather(
            (shared_up * norm_gain_vector[None, :]).astype(jnp.bfloat16), "fs", axis=0, tiled=True
        ),
        lax.all_gather(shared_down.astype(jnp.bfloat16), "fs", axis=0, tiled=True),
    )
    values = tokens.astype(jnp.float32)
    totals = lax.psum(jnp.sum(values * values, axis=1), "tp")
    normed = (values * lax.rsqrt(totals / model_width + norm_eps)[:, None]).astype(jnp.bfloat16)
    flat_expert = routes.reshape(-1)
    onehot = (flat_expert[:, None] == jnp.arange(experts, dtype=jnp.int32)[None, :]).astype(
        jnp.int32
    )
    earlier = jnp.cumsum(onehot, axis=0) - onehot
    slot_index = jnp.sum(earlier * onehot, axis=1)
    target = (flat_expert * capacity + slot_index).reshape(tok_rows, top_count)
    places = jnp.arange(experts * capacity, dtype=jnp.int32)
    placing = jnp.sum(
        (target[:, :, None] == places[None, None, :]).astype(jnp.int32), axis=1
    ).astype(jnp.bfloat16)
    outgoing = lax.dot_general(
        placing, normed, (((0,), (0,)), ((), ())), preferred_element_type=jnp.float32
    ).astype(jnp.bfloat16)
    incoming = lax.all_to_all(
        outgoing.reshape(experts, capacity, portion_width),
        "fs",
        split_axis=0,
        concat_axis=0,
        tiled=True,
    )
    arrived = incoming.reshape(experts * capacity, portion_width)
    partials = (
        dense_rows(arrived, gate_refreshed[0]).astype(jnp.bfloat16),
        dense_rows(arrived, up_new[0]).astype(jnp.bfloat16),
        dense_rows(normed, shared_g).astype(jnp.bfloat16),
        dense_rows(normed, shared_u).astype(jnp.bfloat16),
    )
    gate_part, up_part, sgate_part, sup_part = (
        lax.psum_scatter(partials[0], "tp", scatter_dimension=1, tiled=True).astype(jnp.float32),
        lax.psum_scatter(partials[1], "tp", scatter_dimension=1, tiled=True).astype(jnp.float32),
        lax.psum_scatter(partials[2], "tp", scatter_dimension=1, tiled=True).astype(jnp.float32),
        lax.psum_scatter(partials[3], "tp", scatter_dimension=1, tiled=True).astype(jnp.float32),
    )
    hidden, shared_hidden = (
        lax.all_gather(
            (jax.nn.silu(gate_part) * up_part).astype(jnp.bfloat16), "tp", axis=1, tiled=True
        ),
        lax.all_gather(
            (jax.nn.silu(sgate_part) * sup_part).astype(jnp.bfloat16), "tp", axis=1, tiled=True
        ),
    )
    produced = jnp.dot(hidden, down_new[0], preferred_element_type=jnp.float32).astype(jnp.bfloat16)
    returned = lax.all_to_all(
        produced.reshape(experts, capacity, portion_width),
        "fs",
        split_axis=0,
        concat_axis=0,
        tiled=True,
    )
    picked = returned.reshape(experts * capacity, portion_width)[target]
    routed = jnp.sum(routing_weight[:, :, None] * picked.astype(jnp.float32), axis=1)
    shared_out = jnp.dot(shared_hidden, shared_d, preferred_element_type=jnp.float32)
    mixed = (routed + shared_out).astype(jnp.bfloat16)
    return (mixed, gate_refreshed, up_new, down_new, shared_g, shared_u, shared_d)


MESH = pl.DeviceIdType.MESH


def outward_first(n):
    def key(f):
        return lambda s: (abs(s - f), abs(2 * s - n + 1) <= abs(2 * f - n + 1), s)

    orders = [sorted(range(n), key=key(f)) for f in range(n)]
    return [sum(orders[f][i] * n**f for f in range(n)) for i in range(n)]


def fused_kernel(
    n_fs, n_tp, top_count,
    tok_in, routes_in, weight_in, gain_in, eg_in, eu_in, ed_in, sg_in, su_in, sd_in,
    mixed_ref, wout_ref,
    raw, routes_ref, weight_ref, gain_ref,
    wall, tokbuf, meta_ref, metabuf, ssown, ssbuf, mt, part, rsbuf, hid, part_a, rsbuf_a, hid_a, part_b, rsbuf_b, hid_b, acc, outb, chain,
    in_s, tok_s, tok_r, meta_s, meta_r, ss_s, ss_r, rs_s, rs_r, ag_s, ag_r,
    ch_s, ch_r, we_s, we_r, ws_s, ws_r, yw_s, yw_r,
):
    g, f, t = lax.axis_index("grp"), lax.axis_index("fs"), lax.axis_index("tp")
    rows, width = tokbuf.shape[1:]
    experts, units = eg_in.shape[0], eg_in.shape[1]
    pieces = 3
    row_step = rows // pieces
    half = units // 2
    f32, bf16 = jnp.float32, jnp.bfloat16
    code = outward_first(n_fs)
    scope = jax.named_scope
    parts = [pl.ds(h * row_step, row_step) for h in range(pieces)]
    three = pl.ds(0, n_tp - 1)

    def source(i):
        total = 0
        digits = code[i]
        picks = [(digits // n_fs**q) % n_fs for q in range(n_fs)]
        for q in range(n_fs):
            hit = 1 - jnp.minimum(1, jnp.abs(f - q))
            total = total + picks[q] * hit
        return total

    at_edge = (f == 0) | (f == n_fs - 1)
    inside = (f > 0) & (f < n_fs - 1)

    def at_fs(index):
        return (g, index, t)

    def at_tp(index):
        return (g, f, index)

    partner = (1 - g, f, t)

    def remote(src, dst, send, recv, device):
        return pltpu.make_async_remote_copy(
            src_ref=src, dst_ref=dst, send_sem=send, recv_sem=recv,
            device_id=device, device_id_type=MESH,
        )

    def sent(ref, send):
        remote(ref, ref, send, send, partner).wait_send()

    def landed(ref, recv):
        remote(ref, ref, recv, recv, partner).wait_recv()

    tp_others = [lax.rem(t + j, n_tp) for j in range(1, n_tp)]

    barrier = pltpu.get_barrier_semaphore()

    def greet(device):
        pl.semaphore_signal(barrier, inc=1, device_id=device, device_id_type=MESH)

    @pl.when(f > 0)
    def _():
        greet(at_fs(f - 1))

    @pl.when(f < n_fs - 1)
    def _():
        greet(at_fs(f + 1))

    for device in [at_tp(d) for d in tp_others] + [partner]:
        greet(device)

    small = [
        pltpu.make_async_copy(tok_in, tokbuf.at[f], in_s.at[0]),
        pltpu.make_async_copy(routes_in, routes_ref, in_s.at[1]),
        pltpu.make_async_copy(weight_in, weight_ref, in_s.at[2]),
        pltpu.make_async_copy(gain_in, gain_ref, in_s.at[3]),
    ]
    for load in small:
        load.start()
    for m, (routed, shared) in enumerate(((eg_in, sg_in), (eu_in, su_in), (ed_in, sd_in))):
        pltpu.make_async_copy(routed, raw.at[m, pl.ds(0, experts)], in_s.at[4 + m]).start()
        pltpu.make_async_copy(shared, raw.at[m, experts], in_s.at[4 + m]).start()
    small[0].wait()
    with scope("barrier"):
        pl.semaphore_wait(barrier, n_tp + jnp.minimum(1, f) + jnp.minimum(1, n_fs - 1 - f))

    def convert(m):
        pltpu.make_async_copy(raw.at[m], raw.at[m], in_s.at[4 + m]).wait()
        for e in range(experts + 1):
            value = raw[m, e]
            wall[m, e] = (value * gain_ref[...] if m < 2 else value).astype(bf16)

    def transposed(row_ref):
        return jnp.transpose(row_ref[...])[0:rows]

    segments = [
        (i, 0, rows, part.at[i], rsbuf.at[i], hid.at[i]) for i in range(n_fs - 1)
    ] + [
        (n_fs - 1, 0, 2 * row_step, part_a, rsbuf_a, hid_a),
        (n_fs - 1, 2 * row_step, row_step, part_b, rsbuf_b, hid_b),
    ]

    def forward_block(q):
        i, first, count, part, rsbuf, _ = segments[q]
        span = pl.ds(first, count)
        s = source(i)
        with scope(f"fwd{q}"):
            if first == 0:
                mt[i] = transposed(meta_ref if i == 0 else metabuf.at[s])
            tokens = tokbuf[s, span]
            names = [mt[i, span, k : k + 1] for k in range(top_count)]
            columns = []
            for m in range(2):
                weight = wall[m].reshape((experts + 1) * units, width)
                sums = dense_rows(tokens, weight)
                for name in names:
                    chosen = jnp.zeros((count, units), f32)
                    for e in range(experts):
                        chosen = jnp.where(name == float(e), sums[:, e * units : (e + 1) * units], chosen)
                    columns.append(chosen)
                columns.append(sums[:, experts * units :])
            for c, column in enumerate(columns):
                part[:, :, c * units : (c + 1) * units] = column.astype(bf16).reshape(n_tp, count // n_tp, units)
            for d in tp_others:
                remote(part.at[d], rsbuf.at[t], rs_s.at[0], rs_r.at[q], at_tp(d)).start()

    def hidden_block(q):
        i, first, count, part, rsbuf, hid = segments[q]
        sub = count // n_tp
        with scope(f"hid{q}"):
            weights = mt[i, pl.ds(pl.multiple_of(first + t * sub, 8), sub), :]
            scale = weights[:, 2 * top_count : 2 * top_count + 1]
            landed(rsbuf.at[three], rs_r.at[q])
            total = part[t].astype(f32)
            for d in tp_others:
                total = total + rsbuf[d].astype(f32)
            total = total * scale
            kinds = top_count + 1
            for k in range(kinds):
                gate = total[:, k * units : (k + 1) * units]
                up = total[:, (kinds + k) * units : (kinds + k + 1) * units]
                value = jax.nn.silu(gate) * up
                if k < top_count:
                    value = value * weights[:, top_count + k : top_count + k + 1]
                hid[t, :, k * units : (k + 1) * units] = value.astype(bf16)
            for d in tp_others:
                remote(hid.at[t], hid.at[t], ag_s.at[0], ag_r.at[q], at_tp(d)).start()

    def down_block(q):
        i, first, count, _, _, hid = segments[q]
        span = pl.ds(first, count)
        with scope(f"down{q}"):
            landed(hid.at[three], ag_r.at[q])
            values = hid[...].astype(f32).reshape(count, (top_count + 1) * units)
            names = [mt[i, span, k : k + 1] for k in range(top_count)]
            spread = []
            for e in range(experts):
                chosen = jnp.zeros((count, units), f32)
                for k, name in enumerate(names):
                    chosen = jnp.where(name == float(e), values[:, k * units : (k + 1) * units], chosen)
                spread.append(chosen.astype(bf16))
            spread.append(values[:, top_count * units :].astype(bf16))
            weight = wall[2].reshape((experts + 1) * units, width)
            acc[i, span] = jnp.dot(jnp.concatenate(spread, axis=1), weight, preferred_element_type=f32)

    def chain_send(i, h, hop, last):
        d = source(i)
        slot = d
        if last:
            slot = d + (n_fs - d) * jnp.minimum(1, jnp.maximum(0, f - d))
        remote(
            outb.at[i, parts[h]], chain.at[slot, parts[h]], ch_s.at[0], ch_r.at[slot, h], at_fs(source(hop))
        ).start()

    def chain_start(i, which=(0, 1, 2)):
        for h in which:
            outb[i, parts[h]] = acc[i, parts[h]].astype(bf16)
            chain_send(i, h, 1, i == 1)

    def chain_on(i, h):
        d = source(i)
        with scope(f"chain{i}{h}"):
            landed(chain.at[d, parts[h]], ch_r.at[d, h])
        outb[i, parts[h]] = (acc[i, parts[h]] + chain[d, parts[h]].astype(f32)).astype(bf16)
        chain_send(i, h, min(i, 2), i < 3)

    def chain_end(slot, h):
        with scope(f"last{h}"):
            landed(chain.at[slot, parts[h]], ch_r.at[slot, h])
        acc[0, parts[h]] = acc[0, parts[h]] + chain[slot, parts[h]].astype(f32)

    def tokens_to(hop, s, h):
        ref = tokbuf.at[s, parts[h]]
        remote(ref, ref, tok_s.at[0], tok_r.at[s, h], at_fs(source(hop))).start()

    def meta_to(hop, s):
        remote(
            meta_ref if s is f else metabuf.at[s], metabuf.at[s], meta_s.at[0], meta_r.at[s], at_fs(source(hop))
        ).start()

    def take_tokens(i, h, hop=None):
        s = source(i)
        with scope(f"tok{i}{h}"):
            landed(tokbuf.at[s, parts[h]], tok_r.at[s, h])
            if hop:
                tokens_to(hop, s, h)

    def take_small(i, hop=None):
        s = source(i)
        with scope(f"small{i}"):
            landed(metabuf.at[s], meta_r.at[s])
            if hop:
                meta_to(hop, s)

    mine = pl.ds(pl.multiple_of(g * half, 16), half)

    def give_shared(hop, pieces=(0, 1, 2)):
        for m in pieces:
            remote(
                wall.at[m, experts, mine], wout_ref.at[1, m, f, g], ws_s.at[0], ws_r.at[f, m], at_fs(source(hop))
            ).start()

    def give_expert(i, pieces=(0, 1, 2)):
        d = source(i)
        for m in pieces:
            remote(wall.at[m, d, mine], wout_ref.at[0, m, f, g], we_s.at[0], we_r.at[f, m], at_fs(d)).start()

    def pass_shared(i, m, hop=None):
        s = source(i)
        ref = wout_ref.at[1, m, s, g]
        with scope(f"S{i}{m}"):
            landed(ref, ws_r.at[s, m])
        if hop:
            remote(ref, ref, ws_s.at[0], ws_r.at[s, m], at_fs(source(hop))).start()
        remote(ref, ref, yw_s.at[0], yw_r.at[0], partner).start()

    def pass_routed(i, m):
        s = source(i)
        ref = wout_ref.at[0, m, s, g]
        with scope(f"E{i}{m}"):
            landed(ref, we_r.at[s, m])
        remote(ref, ref, yw_s.at[0], yw_r.at[0], partner).start()

    def start_up(hops):
        for load in small[1:]:
            load.wait()
        meta_ref[...] = jnp.zeros(meta_ref.shape, f32)
        meta_ref[0:top_count, 0:rows] = routes_ref[...].astype(f32)
        meta_ref[top_count : 2 * top_count, 0:rows] = weight_ref[...]
        x = tokbuf[f].astype(f32)
        sq = x * x
        high = sq.astype(bf16)
        low = (sq - high.astype(f32)).astype(bf16)
        ones = jnp.ones((8, width), bf16)
        ssown[...] = jnp.zeros(ssown.shape, f32)
        ssown[:, 0:rows] = dense_rows(ones, high) + dense_rows(ones, low)
        for d in tp_others:
            remote(ssown, ssbuf.at[t], ss_s.at[0], ss_r.at[0], at_tp(d)).start()
        convert(0)
        if len(hops) > 1:
            give_shared(1, (0,))
            give_shared(2, (0,))
        convert(1)
        if len(hops) > 1:
            give_shared(1, (1,))
            tokens_to(1, f, 0)
        forward_block(0)
        squares = ssown[...]
        with scope("sswait"):
            landed(ssbuf.at[three], ss_r.at[0])
        for d in tp_others:
            squares = squares + ssbuf[d]
        scale = lax.rsqrt(squares / (width * n_tp) + norm_eps)
        meta_ref[2 * top_count : 2 * top_count + 1] = scale[0:1]
        for hop in hops:
            meta_to(hop, f)
        mt[0] = transposed(meta_ref)
        convert(2)

    def keep_own():
        for h in range(2):
            wout_ref[0, :, f, h] = wall[:, f, h * half : (h + 1) * half]
            wout_ref[1, :, f, h] = wall[:, experts, h * half : (h + 1) * half]

    def finish():
        mixed_ref[...] = acc[0].astype(bf16)

    @pl.when(at_edge)
    def _():
        for h in range(pieces):
            tokens_to(1, f, h)
        start_up((1,))
        give_shared(1)
        give_expert(1)
        keep_own()
        pass_shared(1, 0)
        pass_shared(1, 1)
        take_tokens(2, 0)
        give_expert(2)
        hidden_block(0)
        take_tokens(2, 1)
        take_tokens(2, 2)
        take_small(2)
        forward_block(2)
        down_block(0)
        pass_shared(1, 2)
        pass_routed(1, 0)
        take_tokens(3, 0)

        @pl.when(f > 0)
        def _():
            give_expert(3)

        pass_routed(1, 1)
        take_tokens(3, 1)
        take_tokens(3, 2)
        take_small(3)

        @pl.when(f == 0)
        def _():
            give_expert(3)

        forward_block(3)
        forward_block(4)
        hidden_block(2)
        pass_routed(3, 0)
        pass_routed(3, 1)
        hidden_block(3)
        hidden_block(4)
        pass_routed(3, 2)
        take_small(1)
        for h in range(pieces):
            take_tokens(1, h)
        forward_block(1)
        pass_routed(1, 2)
        down_block(3)
        chain_start(3, (0, 1))
        pass_shared(2, 0)
        down_block(4)
        chain_start(3, (2,))
        down_block(2)
        chain_start(2)
        pass_shared(2, 1)
        hidden_block(1)
        pass_routed(2, 0)
        pass_routed(2, 1)
        pass_shared(2, 2)
        pass_routed(2, 2)
        down_block(1)
        chain_start(1)
        for m in range(3):
            pass_shared(3, m)
        for h in range(pieces):
            chain_end(f + (n_fs - f) * (1 - jnp.minimum(1, f)), h)
        finish()
        sent(tokbuf.at[0], tok_s.at[0])
        sent(metabuf.at[0], meta_s.at[0])
        sent(wall.at[:, 0, pl.ds(0, half)], ws_s.at[0])

    @pl.when(inside)
    def _():
        for h in range(pieces):
            tokens_to(2, f, h)
        start_up((1, 2))
        for h in range(pieces):
            take_tokens(2, h, hop=1)
            take_tokens(1, h, hop=2)
        take_small(2, hop=1)
        take_small(1, hop=2)
        give_shared(1, (2,))
        give_expert(1, (0, 1))
        give_shared(2, (1, 2))
        give_expert(2)
        forward_block(1)
        forward_block(2)
        hidden_block(0)
        take_tokens(3, 0, hop=1)
        take_tokens(3, 1, hop=1)
        take_tokens(3, 2, hop=1)
        take_small(3, hop=1)
        for h in range(1, pieces):
            tokens_to(1, f, h)
        give_expert(1, (2,))
        forward_block(3)
        forward_block(4)
        keep_own()
        for m in range(3):
            pass_shared(1, m, hop=2)
        give_expert(3)
        hidden_block(1)
        hidden_block(2)
        for m in range(3):
            pass_routed(1, m)
        down_block(0)
        hidden_block(3)
        hidden_block(4)
        pass_shared(2, 0, hop=1)
        pass_shared(2, 1, hop=1)
        down_block(1)
        down_block(2)
        down_block(3)
        down_block(4)
        pass_shared(2, 2, hop=1)
        for m in range(3):
            pass_routed(2, m)
        for m in range(3):
            pass_shared(3, m, hop=1)
        for m in range(3):
            pass_routed(3, m)
        for i, h in ((3, 0), (3, 1), (3, 2), (2, 0), (1, 0), (2, 1), (1, 1), (2, 2), (1, 2)):
            chain_on(i, h)
        for h in range(pieces):
            chain_end(f, h)
            chain_end(n_fs, h)
        finish()
        sent(chain, tok_s.at[0])
        sent(metabuf, meta_s.at[0])
        sent(wall.at[:, :, pl.ds(0, half)], ws_s.at[0])

    with scope("ywait"):
        landed(wout_ref.at[:, :, pl.ds(0, n_fs - 1), 0], yw_r.at[0])

    with scope("drain"):
        sent(ssbuf.at[three], ss_s.at[0])
        sent(part, rs_s.at[0])
        sent(hid, ag_s.at[0])
        sent(outb.at[pl.ds(0, n_fs - 1)], ch_s.at[0])
        sent(wout_ref.at[0, :, pl.ds(0, n_fs - 1), 0], we_s.at[0])
        sent(wout_ref.at[:, :, pl.ds(0, n_fs - 1), 0], yw_s.at[0])


def put_out(mixed_ref, served_ref, *rest):
    outs, sems = rest[:-1], rest[-1]
    step = served_ref.shape[1] // 4
    for i in range(len(outs) - 1):
        for j in range(4):
            span = pl.ds(j * step, step)
            pltpu.make_async_copy(served_ref.at[i, span], outs[1 + i].at[span], sems.at[1 + i]).start()
    pltpu.make_async_copy(mixed_ref, outs[0], sems.at[0]).start()
    for i in range(len(outs) - 1):
        pltpu.make_async_copy(served_ref.at[i], outs[1 + i], sems.at[1 + i]).wait()
    pltpu.make_async_copy(mixed_ref, outs[0], sems.at[0]).wait()


def per_device_fused(
    tokens,
    routes,
    routing_weight,
    norm_gain_vector,
    expert_gate,
    expert_up,
    expert_down,
    shared_gate,
    shared_up,
    shared_down,
):
    n_fs, n_tp = lax.axis_size("fs"), lax.axis_size("tp")
    rows, width = tokens.shape
    experts, units, _ = expert_gate.shape
    top_count = routes.shape[1]
    half = units // 2
    meta_rows = -(-(2 * top_count + 1) // 8) * 8
    lanes = -(-rows // 128) * 128
    f32, bf16 = jnp.float32, jnp.bfloat16
    kinds = top_count + 1
    dma = pltpu.SemaphoreType.DMA
    vmem = pl.BlockSpec(memory_space=pltpu.VMEM)
    hbm = pl.BlockSpec(memory_space=pltpu.HBM)
    mixed, served = pl.pallas_call(
        functools.partial(fused_kernel, n_fs, n_tp, top_count),
        out_shape=(
            pltpu.VMEM((rows, width), bf16),
            pltpu.VMEM((2, 3, n_fs, 2, half, width), bf16),
        ),
        in_specs=[hbm] * 10,
        out_specs=(vmem, vmem),
        scratch_shapes=[
            pltpu.VMEM((3, experts + 1, units, width), f32),
            pltpu.VMEM((top_count, rows), jnp.int32),
            pltpu.VMEM((top_count, rows), f32),
            pltpu.VMEM((1, width), f32),
            pltpu.VMEM((3, experts + 1, units, width), bf16),
            pltpu.VMEM((n_fs, rows, width), bf16),
            pltpu.VMEM((meta_rows, lanes), f32),
            pltpu.VMEM((n_fs + 1, meta_rows, lanes), f32),
            pltpu.VMEM((8, lanes), f32),
            pltpu.VMEM((n_tp, 8, lanes), f32),
            pltpu.VMEM((n_fs, rows, meta_rows), f32),
            *[
                pltpu.VMEM(lead + (n_tp, count // n_tp, times * kinds * units), bf16)
                for lead, count in (((n_fs - 1,), rows), ((), 2 * rows // 3), ((), rows // 3))
                for times in (2, 2, 1)
            ],
            pltpu.VMEM((n_fs, rows, width), f32),
            pltpu.VMEM((n_fs, rows, width), bf16),
            pltpu.VMEM((n_fs + 1, rows, width), bf16),
            dma((7,)),
            dma((1,)), dma((n_fs, 3)),
            dma((1,)), dma((n_fs,)),
            dma((1,)), dma((1,)),
            dma((1,)), dma((n_fs + 1,)),
            dma((1,)), dma((n_fs + 1,)),
            dma((1,)), dma((n_fs + 1, 3)),
            dma((1,)), dma((n_fs, 3)),
            dma((1,)), dma((n_fs, 3)),
            dma((1,)), dma((1,)),
        ],
        compiler_params=pltpu.CompilerParams(
            collective_id=0, has_side_effects=True, vmem_limit_bytes=40 * 1024 * 1024
        ),
        name="hand_over_and_layer",
    )(*[
        pltpu.with_memory_space_constraint(value, pltpu.HBM)
        for value in (
            tokens, routes.T, routing_weight.T, norm_gain_vector[None, :],
            expert_gate, expert_up, expert_down, shared_gate, shared_up, shared_down,
        )
    ])
    units_all = n_fs * units
    outs = pl.pallas_call(
        put_out,
        out_shape=(
            jax.ShapeDtypeStruct((rows, width), bf16),
            *[jax.ShapeDtypeStruct((units_all, width), bf16)] * 6,
        ),
        in_specs=[vmem] * 2,
        out_specs=(hbm,) * 7,
        scratch_shapes=[dma((7,))],
        compiler_params=pltpu.CompilerParams(vmem_limit_bytes=8 * 1024 * 1024),
        name="put_out",
    )(mixed, served.reshape(6, units_all, width))
    return (outs[0], outs[1][None], outs[2][None], outs[3][None], *outs[4:])


def per_device(tokens, routes, routing_weight, norm_gain_vector, *weights):
    experts, units, width = weights[0].shape
    rows, n_fs, n_tp = tokens.shape[0], lax.axis_size("fs"), lax.axis_size("tp")
    whole_tiles = units % 128 == 0 and width % 128 == 0 and rows % (48 * n_tp) == 0
    fits = (experts + 1) * units * width <= 2**20 and n_fs == 4 and n_tp <= 4
    chosen = per_device_plain
    if whole_tiles and fits and experts == n_fs and lax.axis_size("grp") == 2:
        chosen = per_device_fused
    return chosen(tokens, routes, routing_weight, norm_gain_vector, *weights)


def solution(mesh):
    return jax.shard_map(
        per_device,
        mesh=mesh,
        in_specs=(
            P(("grp", "fs"), "tp"),
            P(("grp", "fs"), None),
            P(("grp", "fs"), None),
            P("tp"),
            P(None, "fs", "tp"),
            P(None, "fs", "tp"),
            P(None, "fs", "tp"),
            P("fs", "tp"),
            P("fs", "tp"),
            P("fs", "tp"),
        ),
        out_specs=(
            P(("grp", "fs"), "tp"),
            P(("grp", "fs"), None, "tp"),
            P(("grp", "fs"), None, "tp"),
            P(("grp", "fs"), None, "tp"),
            P("grp", "tp"),
            P("grp", "tp"),
            P("grp", "tp"),
        ),
        check_vma=False,
    )
```
